32 devices in a mesh: grp: 2 (over y), sp: 4 (over z), tp: 4 (over x, core).
Axes of the slice: x: 2, y: 2, z: 4, core: 2. Of those that a mesh axis runs over, the one named last changes fastest.
Arguments:
- residual_in: bfloat16 [2048, 2048], P(('grp', 'sp', 'tp')), parts along dimension 0, may hold values from -6 to 6
- q_small: bfloat16 [2048, 1024], P(('grp', 'sp'), 'tp'), parts along dimension 0, may hold values from -5 to 5
- k_small: bfloat16 [2048, 256], P(('grp', 'sp'), 'tp'), parts along dimension 0, may hold values from -5 to 5
- v_small: bfloat16 [2048, 256], P(('grp', 'sp'), 'tp'), parts along dimension 0, may hold values from -6 to 6
- q_large: bfloat16 [2048, 1024], P(('grp', 'sp'), 'tp'), parts along dimension 0, may hold values from -5 to 5
- k_large: bfloat16 [2048, 512], P(('grp', 'sp'), 'tp'), parts along dimension 0, may hold values from -5 to 5
- v_large: bfloat16 [2048, 512], P(('grp', 'sp'), 'tp'), parts along dimension 0, may hold values from -6 to 6
- gain_qs: float32 [64], replicated, may hold values from 0.24 to 7.4
- gain_ks: float32 [64], replicated, may hold values from 0.24 to 7.4
- gain_ql: float32 [128], replicated, may hold values from 0.24 to 7.4
- gain_kl: float32 [128], replicated, may hold values from 0.24 to 7.4
- w_out_small: bfloat16 [1024, 2048], P('tp'), may hold values from -0.125 to 0.125
- w_out_large: bfloat16 [1024, 2048], P('tp'), may hold values from -0.125 to 0.125
- g_ffn: float32 [2048], replicated, may hold values from 0.1 to 1.9
- routes: int32 [2048, 4], P(('grp', 'sp', 'tp')), parts along dimension 0, may hold values from 0 to 7, all different within a row; in each aligned block of 64 rows (0 to 63, 64 to 127, ...) at most 64 rows name the same one
- route_w: float32 [2048, 4], P(('grp', 'sp', 'tp')), parts along dimension 0, may hold values from 0.2 to 1
- w_gate: bfloat16 [8, 2048, 1024], P('sp', None, 'tp'), may hold values from -0.125 to 0.125
- w_up: bfloat16 [8, 2048, 1024], P('sp', None, 'tp'), may hold values from -0.125 to 0.125
- w_down: bfloat16 [8, 1024, 2048], P('sp', 'tp'), may hold values from -0.1875 to 0.1875
- ws_gate: bfloat16 [2048, 1024], P(None, 'tp'), may hold values from -0.125 to 0.125
- ws_up: bfloat16 [2048, 1024], P(None, 'tp'), may hold values from -0.125 to 0.125
- ws_down: bfloat16 [1024, 2048], P('tp'), may hold values from -0.1875 to 0.1875
Outputs:
- result: bfloat16 [2048, 2048], P(('grp', 'sp', 'tp')), parts along dimension 0
The draws below stay inside these ranges and needn't reach their ends.
There are 2 independent parts, one for each index of `grp`. The reference program is written for one: setup_inputs(seed, part) draws one part's arguments, and reference() takes and returns one part's arrays. A program takes and returns all parts, laid end to end along the dimension named above; an argument that names none is the same for every part. Nothing has to cross between parts.
Inputs may be any that keep to these rules, and one draw needn't show every extreme that they name: `routes`: each row names 4 different experts. Among the rows of one device no expert is named more than 64 times, a bound that some block reaches.
All inputs are finite; a program needn't handle non-finite values.
Results may differ from the reference program's by a relative error of at most 0.018.
The reference program's roundings to bfloat16 on the way count: a program that leaves them out, or rounds other values in their place, can miss the bound.
Values may be sent and summed in bfloat16 or wider, within the bound.
A program may use at most 128 MiB of HBM per device.

```python
import math
import jax
import jax.numpy as jnp
import numpy as np
from jax import lax

D = 2048
QA = 16
HS_SMALL = 64
KVA = 4
QB = 8
HS_LARGE = 128
KVB = 4
FF = 1024
FF_SH = 1024
GRID_W = 64
TOPK = 4
TOKENS = 1024
ROWS_DEV = 64
EXPERTS = 8
CAP = 64
N_SP = 4
N_TP = 4


def paired_heads(key, kv_heads, head_width, query_heads):
    key_rows = jax.random.normal(jax.random.fold_in(key, 701 + head_width), (TOKENS, kv_heads, head_width), jnp.float32)
    queries = jax.random.normal(jax.random.fold_in(key, 702 + head_width), (TOKENS, kv_heads, query_heads // kv_heads, head_width), jnp.float32)
    queries = jnp.clip(queries, -5.0, 5.0)
    key_rows = jnp.clip(key_rows, -5.0, 5.0)
    return (queries.reshape(TOKENS, query_heads * head_width), key_rows.reshape(TOKENS, kv_heads * head_width))


def positive_gain(key, channels, salt):
    return jnp.exp(jax.random.uniform(jax.random.fold_in(key, salt), (channels,), jnp.float32, -1.4, 1.4))


def draw_q_small(key, part):
    return paired_heads(key, KVA, HS_SMALL, QA)[0].astype(jnp.bfloat16)


def draw_k_small(key, part):
    return paired_heads(key, KVA, HS_SMALL, QA)[1].astype(jnp.bfloat16)


def draw_q_large(key, part):
    return paired_heads(key, KVB, HS_LARGE, QB)[0].astype(jnp.bfloat16)


def draw_k_large(key, part):
    return paired_heads(key, KVB, HS_LARGE, QB)[1].astype(jnp.bfloat16)


def draw_gain_qs(key, part):
    return positive_gain(key, HS_SMALL, 811)


def draw_gain_ks(key, part):
    return positive_gain(key, HS_SMALL, 812)


def draw_gain_ql(key, part):
    return positive_gain(key, HS_LARGE, 813)


def draw_gain_kl(key, part):
    return positive_gain(key, HS_LARGE, 814)


def levels(key, shape, shards, low, top_value):
    loudness, own = 1.0, jax.random.fold_in(key, 6)
    for dim, shards_of in shards:
        heights = jnp.exp(jax.random.uniform(jax.random.fold_in(own, dim), (shards_of,), jnp.float32, low / len(shards), top_value / len(shards)))
        loudness = loudness * jnp.repeat(heights, shape[dim] // shards_of).reshape([-1 if axis == dim else 1 for axis in range(len(shape))])
    return loudness


def deal_out(key, own, number, rows, amount, top, bound, skew):
    sequence = jax.random.permutation(key, amount)
    heavy_load, usual = load_shares(amount, rows * top, bound, skew, True), load_shares(amount, rows * top, bound, skew, False)
    places = jnp.arange(amount)

    def named(tallies, turn):
        used = int((tallies > 0).sum())
        fixed = max(1, used // 4)
        moved = fixed + (places - fixed + turn * (used - fixed)) % max(1, amount - fixed)
        return jnp.zeros((amount,), jnp.int32).at[sequence[jnp.where(places < fixed, places, moved)]].set(jnp.asarray(tallies, jnp.int32))

    tallies = jnp.where(number % 4 == 0, named(heavy_load, number // 4), named(usual, number - number // 4 - 1))
    mixed = jax.random.permutation(jax.random.fold_in(own, 3), amount)
    giver, taker = mixed[0:amount // 2 * 2:2], mixed[1:amount // 2 * 2:2]
    margin = jnp.minimum(tallies[giver] - 1, bound - tallies[taker]) // 2
    margin = jnp.where((giver == sequence[0]) | (taker == sequence[0]) | (tallies[taker] == 0), 0, jnp.maximum(margin, 0))
    moved = jax.random.randint(jax.random.fold_in(own, 4), (amount // 2,), 0, 1 << 20) % (margin + 1)
    tallies = tallies.at[giver].add(-moved).at[taker].add(moved)
    items = jnp.searchsorted(jnp.cumsum(tallies), jnp.arange(rows * top), side="right").astype(jnp.int32)
    table = items.reshape(top, rows).T
    table = table[jax.random.permutation(jax.random.fold_in(own, 1), rows)]
    turn = jax.random.randint(jax.random.fold_in(own, 2), (rows, 1), 0, top)
    return jnp.take_along_axis(table, (jnp.arange(top)[None, :] + turn) % top, axis=1)


def load_shares(number_of, total, limit, skew, full):
    loads = [(1 << 20) // math.isqrt(rank ** skew) + 1 for rank in range(1, number_of + 1)]
    largest = limit if full else min(limit, max(-(-total // number_of), total * loads[0] // sum(loads)))
    least = 1 if total - largest >= number_of - 1 else 0
    holding, rest = [largest] + [least] * (number_of - 1), total - largest - least * (number_of - 1)
    while rest > 0:
        candidates = [i for i in range(1, number_of) if holding[i] < largest] or [i for i in range(1, number_of) if holding[i] < limit]
        pool, budget = sum([loads[i] for i in candidates]), rest
        for i in candidates:
            addition = min(limit - holding[i], max(1, budget * loads[i] // pool), rest)
            holding[i] = holding[i] + addition
            rest = rest - addition
    return np.array(holding)


def scatter_about(stream_key, shape, spread, bound, cuts=(), kind=jnp.bfloat16):
    level = levels(stream_key, shape, cuts, -0.22, 0.18) if cuts else 1.0
    entries = jax.random.normal(stream_key, shape, jnp.float32) * spread * level
    return jnp.minimum(jnp.maximum(entries, -bound), bound).astype(kind)


def setup_inputs(seed: int = 0, part: int = 0) -> dict:
    splits = jax.random.split(jax.random.key(seed), 23)
    part_keys = jax.random.split(jax.random.fold_in(splits[22], part), 23)
    residual_in = scatter_about(part_keys[0], (TOKENS, D), 1.0, 6.0, ((0, 16),))
    q_small = draw_q_small(jax.random.fold_in(jax.random.fold_in(splits[22], part), 71), part)
    k_small = draw_k_small(jax.random.fold_in(jax.random.fold_in(splits[22], part), 71), part)
    v_small = scatter_about(part_keys[3], (TOKENS, KVA * HS_SMALL), 1.0, 6.0, ((0, 4), (1, 4)))
    q_large = draw_q_large(jax.random.fold_in(jax.random.fold_in(splits[22], part), 71), part)
    k_large = draw_k_large(jax.random.fold_in(jax.random.fold_in(splits[22], part), 71), part)
    v_large = scatter_about(part_keys[6], (TOKENS, KVB * HS_LARGE), 1.0, 6.0, ((0, 4), (1, 4)))
    gain_qs = draw_gain_qs(jax.random.fold_in(splits[22], 71), part)
    gain_ks = draw_gain_ks(jax.random.fold_in(splits[22], 71), part)
    gain_ql = draw_gain_ql(jax.random.fold_in(splits[22], 71), part)
    gain_kl = draw_gain_kl(jax.random.fold_in(splits[22], 71), part)
    w_out_small = scatter_about(splits[11], (QA * HS_SMALL, D), (QA * HS_SMALL + QB * HS_LARGE) ** -0.5, 0.125, ((0, 4),))
    w_out_large = scatter_about(splits[12], (QB * HS_LARGE, D), (QA * HS_SMALL + QB * HS_LARGE) ** -0.5, 0.125, ((0, 4),))
    g_ffn = jnp.clip(1.0 + 0.18 * jax.random.normal(splits[13], (D,), jnp.float32), 0.1, 1.9)
    routes_keys = jax.random.split(jax.random.fold_in(part_keys[14], 1), TOKENS // ROWS_DEV)
    routes_turns = jax.random.permutation(jax.random.fold_in(part_keys[14], 3), TOKENS // ROWS_DEV)
    routes = jax.vmap(lambda own, number: deal_out(jax.random.fold_in(part_keys[14], 2), own, number, ROWS_DEV, EXPERTS, TOPK, CAP, 2))(routes_keys, routes_turns).reshape((TOKENS, TOPK))
    route_w = jnp.clip(0.2 + 0.8 * jax.random.uniform(part_keys[15], (TOKENS, TOPK), jnp.float32) ** levels(part_keys[15], (TOKENS, TOPK), ((0, 16),), -0.2, 0.2), 0.2, 1.0)
    w_gate = scatter_about(splits[16], (EXPERTS, D, FF), D ** -0.5, 0.125, ((0, 4), (2, 4)))
    w_up = scatter_about(splits[17], (EXPERTS, D, FF), D ** -0.5, 0.125, ((0, 4), (2, 4)))
    w_down = scatter_about(splits[18], (EXPERTS, FF, D), FF ** -0.5, 0.1875, ((0, 4), (1, 4)))
    ws_gate = scatter_about(splits[19], (D, FF_SH), D ** -0.5, 0.125, ((1, 4),))
    ws_up = scatter_about(splits[20], (D, FF_SH), D ** -0.5, 0.125, ((1, 4),))
    ws_down = scatter_about(splits[21], (FF_SH, D), FF_SH ** -0.5, 0.1875, ((0, 4),))
    return {"residual_in": residual_in, "q_small": q_small, "k_small": k_small, "v_small": v_small, "q_large": q_large, "k_large": k_large, "v_large": v_large, "gain_qs": gain_qs, "gain_ks": gain_ks, "gain_ql": gain_ql, "gain_kl": gain_kl, "w_out_small": w_out_small, "w_out_large": w_out_large, "g_ffn": g_ffn, "routes": routes, "route_w": route_w, "w_gate": w_gate, "w_up": w_up, "w_down": w_down, "ws_gate": ws_gate, "ws_up": ws_up, "ws_down": ws_down}


norm_eps = 1e-06
rope_base = 10000.0

def rounded(values):
    return lax.optimization_barrier(values.astype(jnp.bfloat16)).astype(jnp.float32)

def rotate_pairs(values, angles):
    front_half, back_half = jnp.split(values, 2, axis=-1)
    cosine_vals = jnp.cos(angles)[:, None, :]
    sine_vals = jnp.sin(angles)[:, None, :]
    return jnp.concatenate([front_half * cosine_vals - back_half * sine_vals, front_half * sine_vals + back_half * cosine_vals], axis=-1)

def norm_rotate(heads_in, gain, positions, grid_width):
    channels = gain.shape[0]
    values = heads_in.astype(jnp.float32).reshape(heads_in.shape[0], -1, channels)
    values = values * lax.rsqrt(lax.optimization_barrier(jnp.mean(values * values, axis=-1, keepdims=True)) + norm_eps) * gain
    quarter = channels // 4
    inverse = 1.0 / rope_base ** (jnp.arange(quarter, dtype=jnp.float32) / quarter)
    grid_rows = (positions // grid_width).astype(jnp.float32)
    grid_cols = (positions % grid_width).astype(jnp.float32)
    half_width = channels // 2
    turned = jnp.concatenate([rotate_pairs(values[..., :half_width], grid_rows[:, None] * inverse[None, :]), rotate_pairs(values[..., half_width:], grid_cols[:, None] * inverse[None, :])], axis=-1)
    return turned.astype(jnp.bfloat16)

def attend(queries, key_rows, value_rows):
    tokens, heads, channels = queries.shape
    kv_heads = key_rows.shape[1]
    group = heads // kv_heads
    block_rows = math.gcd(tokens, 256)
    blocks = queries.reshape(tokens // block_rows, block_rows, kv_heads, group, channels)
    keys32 = key_rows.astype(jnp.float32)
    values32 = value_rows.astype(jnp.float32)

    def one_block(query_block):
        scores = jnp.einsum('qkgd,skd->kgqs', query_block.astype(jnp.float32), keys32) * channels ** (-0.5)
        peak_val = lax.optimization_barrier(jnp.max(scores, axis=-1, keepdims=True))
        weights_raw = jnp.exp(scores - peak_val)
        totals = lax.optimization_barrier(jnp.sum(weights_raw, axis=-1))
        weights = rounded(weights_raw)
        mixture = jnp.einsum('kgqs,skd->qkgd', weights, values32)
        mixture = mixture / jnp.transpose(totals, (2, 0, 1))[..., None]
        return mixture.astype(jnp.bfloat16)
    result = lax.map(one_block, blocks)
    return result.reshape(tokens, heads * channels)

def split_down(hidden, down_w, pieces):
    columns = hidden.shape[1] // pieces
    summed = jnp.zeros((hidden.shape[0], down_w.shape[1]), jnp.float32)
    for device in range(pieces):
        term = jnp.dot(hidden[:, device * columns:(device + 1) * columns], down_w[device * columns:(device + 1) * columns], preferred_element_type=jnp.float32)
        summed = summed + rounded(term)
    return summed

def reference(residual_in, q_small, k_small, v_small, q_large, k_large, v_large, gain_qs, gain_ks, gain_ql, gain_kl, w_out_small, w_out_large, g_ffn, routes, route_w, w_gate, w_up, w_down, ws_gate, ws_up, ws_down):
    positions = jnp.arange(TOKENS, dtype=jnp.int32)
    heads_small = attend(norm_rotate(q_small, gain_qs, positions, GRID_W), norm_rotate(k_small, gain_ks, positions, GRID_W), v_small.reshape(TOKENS, KVA, HS_SMALL))
    heads_large = attend(norm_rotate(q_large, gain_ql, positions, GRID_W), norm_rotate(k_large, gain_kl, positions, GRID_W), v_large.reshape(TOKENS, KVB, HS_LARGE))
    small_cols = QA * HS_SMALL // N_TP
    large_cols = QB * HS_LARGE // N_TP
    head_sum = jnp.zeros((TOKENS, D), jnp.float32)
    for device in range(N_TP):
        term = jnp.dot(heads_small[:, device * small_cols:(device + 1) * small_cols], w_out_small[device * small_cols:(device + 1) * small_cols], preferred_element_type=jnp.float32)
        term = term + jnp.dot(heads_large[:, device * large_cols:(device + 1) * large_cols], w_out_large[device * large_cols:(device + 1) * large_cols], preferred_element_type=jnp.float32)
        head_sum = head_sum + rounded(term)
    stream32 = rounded(residual_in.astype(jnp.float32) + head_sum)
    normed = (stream32 * lax.rsqrt(lax.optimization_barrier(jnp.mean(stream32 * stream32, axis=-1, keepdims=True)) + norm_eps) * g_ffn).astype(jnp.bfloat16)
    assigned = TOKENS * TOPK
    flat_ids = routes.reshape(assigned)
    flat_weights = jnp.concatenate([route_w.reshape(assigned), jnp.zeros((1,), jnp.float32)])
    padded_rows = jnp.concatenate([normed, jnp.zeros((1, D), jnp.bfloat16)], axis=0)
    most_rows = N_SP * N_TP * CAP

    def one_expert(routed, inputs):
        expert, gate_w, up_w, down_w = inputs
        picked = jnp.nonzero(flat_ids == expert, size=most_rows, fill_value=assigned)[0].astype(jnp.int32)
        owners = jnp.where(picked < assigned, picked // TOPK, TOKENS).astype(jnp.int32)
        rows_in = padded_rows[owners]
        gate_act = jnp.dot(rows_in, gate_w, preferred_element_type=jnp.float32)
        up_act = jnp.dot(rows_in, up_w, preferred_element_type=jnp.float32)
        hidden = (jax.nn.silu(gate_act) * up_act).astype(jnp.bfloat16)
        expert_out = split_down(hidden, down_w, N_TP).astype(jnp.bfloat16)
        routed = routed.at[owners].add(flat_weights[picked][:, None] * expert_out.astype(jnp.float32))
        return (routed, None)
    routed, _ = lax.scan(one_expert, jnp.zeros((TOKENS + 1, D), jnp.float32), (jnp.arange(EXPERTS, dtype=jnp.int32), w_gate, w_up, w_down))
    shared_hidden = (jax.nn.silu(jnp.dot(normed, ws_gate, preferred_element_type=jnp.float32)) * jnp.dot(normed, ws_up, preferred_element_type=jnp.float32)).astype(jnp.bfloat16)
    shared = split_down(shared_hidden, ws_down, N_TP)
    return (stream32 + routed[:TOKENS] + shared).astype(jnp.bfloat16)
```

```python
import functools
import math

import jax
import jax.numpy as jnp
from jax import lax
from jax.experimental import pallas as pl
from jax.experimental.pallas import tpu as pltpu
from jax.sharding import PartitionSpec as P

GRID_W = 64
TOPK = 4


norm_eps = 1e-06
rope_base = 10000.0
far_below = -1e30


def rotate_pairs(values, angles):
    front_half, back_half = jnp.split(values, 2, axis=-1)
    cosine_vals = jnp.cos(angles)[:, None, :]
    sine_vals = jnp.sin(angles)[:, None, :]
    return jnp.concatenate(
        [
            front_half * cosine_vals - back_half * sine_vals,
            front_half * sine_vals + back_half * cosine_vals,
        ],
        axis=-1,
    )


def norm_rotate(heads_in, gain, positions, grid_width):
    channels = gain.shape[0]
    values = heads_in.astype(jnp.float32).reshape(heads_in.shape[0], -1, channels)
    values = values * lax.rsqrt(jnp.mean(values * values, axis=-1, keepdims=True) + norm_eps) * gain
    quarter = channels // 4
    inverse = 1.0 / rope_base ** (jnp.arange(quarter, dtype=jnp.float32) / quarter)
    grid_rows = (positions // grid_width).astype(jnp.float32)
    grid_cols = (positions % grid_width).astype(jnp.float32)
    half_width = channels // 2
    turned = jnp.concatenate(
        [
            rotate_pairs(values[..., :half_width], grid_rows[:, None] * inverse[None, :]),
            rotate_pairs(values[..., half_width:], grid_cols[:, None] * inverse[None, :]),
        ],
        axis=-1,
    )
    return turned.astype(jnp.bfloat16)


def absorb(carried, segment, queries):
    peak_val, totals, mixture = carried
    kv_heads = queries.shape[1]
    channels = queries.shape[3]
    pairs = segment.reshape(segment.shape[0], 2, kv_heads, channels)
    scores = jnp.einsum(
        "qkgd,skd->kgqs", queries, pairs[:, 0], preferred_element_type=jnp.float32
    ) * channels ** (-0.5)
    new_peak = jnp.maximum(peak_val, jnp.max(scores, axis=-1))
    weights_raw = jnp.exp(scores - new_peak[..., None])
    shrink = jnp.exp(peak_val - new_peak)
    totals = totals * shrink + jnp.sum(weights_raw, axis=-1)
    update = jnp.einsum(
        "kgqs,skd->qkgd",
        weights_raw.astype(jnp.bfloat16),
        pairs[:, 1],
        preferred_element_type=jnp.float32,
    )
    mixture = mixture * jnp.transpose(shrink, (2, 0, 1))[..., None] + update
    return (new_peak, totals, mixture)


def absorb_blocks(carried, segment, queries):
    row_count = segment.shape[0]
    block_rows = math.gcd(row_count, 1024)
    stacked = segment.reshape(row_count // block_rows, block_rows, segment.shape[1])

    def fold_step(inner, key_block):
        return (absorb(inner, key_block, queries), None)

    carried, _ = lax.scan(fold_step, carried, stacked)
    return carried


def start_state(queries):
    local_rows, kv_heads, group, channels = queries.shape
    return (
        jnp.full((kv_heads, group, local_rows), far_below, jnp.float32),
        jnp.zeros((kv_heads, group, local_rows), jnp.float32),
        jnp.zeros(queries.shape, jnp.float32),
    )


def finish(carried):
    peak_val, totals, mixture = carried
    heads_out = mixture / jnp.transpose(totals, (2, 0, 1))[..., None]
    return heads_out.reshape(heads_out.shape[0], -1).astype(jnp.bfloat16)


def local(
    residual_in,
    q_small,
    k_small,
    v_small,
    q_large,
    k_large,
    v_large,
    gain_qs,
    gain_ks,
    gain_ql,
    gain_kl,
    w_out_small,
    w_out_large,
    g_ffn,
    routes,
    route_w,
    w_gate,
    w_up,
    w_down,
    ws_gate,
    ws_up,
    ws_down,
):
    local_rows = q_small.shape[0]
    positions = lax.axis_index("sp") * local_rows + jnp.arange(local_rows, dtype=jnp.int32)
    query_small = norm_rotate(q_small, gain_qs, positions, GRID_W)
    key_small = norm_rotate(k_small, gain_ks, positions, GRID_W)
    query_large = norm_rotate(q_large, gain_ql, positions, GRID_W)
    key_large = norm_rotate(k_large, gain_kl, positions, GRID_W)
    query_small = query_small.reshape(local_rows, key_small.shape[1], -1, gain_qs.shape[0])
    query_large = query_large.reshape(local_rows, key_large.shape[1], -1, gain_ql.shape[0])
    pack_small = jnp.concatenate([key_small.reshape(local_rows, -1), v_small], axis=1)
    pack_large = jnp.concatenate([key_large.reshape(local_rows, -1), v_large], axis=1)
    segment = (
        lax.all_gather(pack_small, "sp", axis=0, tiled=True),
        lax.all_gather(pack_large, "sp", axis=0, tiled=True),
    )
    heads_small = finish(absorb_blocks(start_state(query_small), segment[0], query_small))
    heads_large = finish(absorb_blocks(start_state(query_large), segment[1], query_large))
    tp_count = lax.axis_size("tp")
    sp_count = lax.axis_size("sp")
    rows_dev = local_rows // tp_count
    head_sum = lax.psum_scatter(
        (
            jnp.dot(heads_small, w_out_small, preferred_element_type=jnp.float32)
            + jnp.dot(heads_large, w_out_large, preferred_element_type=jnp.float32)
        ).astype(jnp.bfloat16),
        "tp",
        scatter_dimension=0,
        tiled=True,
    ).astype(jnp.float32)
    stream = (residual_in.astype(jnp.float32) + head_sum).astype(jnp.bfloat16)
    stream32 = lax.optimization_barrier(stream).astype(jnp.float32)
    normed = (
        stream32
        * lax.rsqrt(jnp.mean(stream32 * stream32, axis=-1, keepdims=True) + norm_eps)
        * g_ffn
    ).astype(jnp.bfloat16)
    channels = normed.shape[1]
    segment = lax.all_gather(normed, "tp", axis=0, tiled=True)
    gate_act = jnp.dot(segment, ws_gate, preferred_element_type=jnp.float32)
    up_act = jnp.dot(segment, ws_up, preferred_element_type=jnp.float32)
    hidden_shared = (jax.nn.silu(gate_act) * up_act).astype(jnp.bfloat16)
    shared = lax.psum_scatter(
        jnp.dot(hidden_shared, ws_down, preferred_element_type=jnp.float32).astype(jnp.bfloat16),
        "tp",
        scatter_dimension=0,
        tiled=True,
    ).astype(jnp.float32)
    local_experts = w_gate.shape[0]
    experts = local_experts * sp_count
    capacity = max(2, 2 * rows_dev * TOPK // experts)
    flat_ids = routes.reshape(-1)
    one_hot = (flat_ids[:, None] == jnp.arange(experts, dtype=jnp.int32)[None, :]).astype(jnp.int32)
    slot_ids = jnp.sum((jnp.cumsum(one_hot, axis=0) - 1) * one_hot, axis=1)
    targets = flat_ids * capacity + slot_ids
    owners = jnp.arange(rows_dev * TOPK, dtype=jnp.int32) // TOPK
    outbox = jnp.zeros((experts * capacity, channels), jnp.bfloat16).at[targets].set(normed[owners])
    arrived = lax.all_to_all(outbox, "sp", split_axis=0, concat_axis=0, tiled=True)
    arrived = lax.all_gather(
        arrived.reshape(sp_count, 1, local_experts, capacity, channels), "tp", axis=1, tiled=True
    )
    gate_act = jnp.einsum("abecd,edf->abecf", arrived, w_gate, preferred_element_type=jnp.float32)
    up_act = jnp.einsum("abecd,edf->abecf", arrived, w_up, preferred_element_type=jnp.float32)
    hidden = (jax.nn.silu(gate_act) * up_act).astype(jnp.bfloat16)
    partial_value = jnp.einsum(
        "abecf,efd->abecd", hidden, w_down, preferred_element_type=jnp.float32
    )
    summed = lax.psum_scatter(
        partial_value.astype(jnp.bfloat16), "tp", scatter_dimension=1, tiled=True
    )
    returned = lax.all_to_all(
        summed.reshape(sp_count * local_experts * capacity, channels),
        "sp",
        split_axis=0,
        concat_axis=0,
        tiled=True,
    )
    picked = returned[targets].reshape(rows_dev, TOPK, channels).astype(jnp.float32)
    routed = jnp.sum(picked * route_w[..., None], axis=1)
    return (stream32 + routed + shared).astype(jnp.bfloat16)


MESH = pl.DeviceIdType.MESH


def greet(peers):
    barrier = pltpu.get_barrier_semaphore()
    for peer in peers:
        pl.semaphore_signal(barrier, inc=1, device_id=peer, device_id_type=MESH)
    pl.semaphore_wait(barrier, len(peers))


def remote(src, dst, send, recv, peer):
    return pltpu.make_async_remote_copy(
        src_ref=src, dst_ref=dst, send_sem=send, recv_sem=recv, device_id=peer, device_id_type=MESH
    )


def gather_kernel(n, pack_ref, out_ref, send, recv):
    me = lax.axis_index("sp")
    peers = [{"sp": lax.rem(me + k, n)} for k in range(1, n)]
    greet(peers)
    copies = [
        remote(pack_ref, out_ref.at[me], send.at[k], recv.at[k], peer)
        for k, peer in enumerate(peers)
    ]
    for copy in copies:
        copy.start()
    out_ref[me] = pack_ref[...]
    for copy in copies:
        copy.wait()


def gather_rows(pack):
    n = lax.axis_size("sp")
    rows, width = pack.shape
    gathered = pl.pallas_call(
        functools.partial(gather_kernel, n),
        out_shape=jax.ShapeDtypeStruct((n, rows, width), pack.dtype),
        in_specs=[pl.BlockSpec(memory_space=pltpu.VMEM)],
        out_specs=pl.BlockSpec(memory_space=pltpu.VMEM),
        scratch_shapes=[pltpu.SemaphoreType.DMA((n - 1,)), pltpu.SemaphoreType.DMA((n - 1,))],
        compiler_params=pltpu.CompilerParams(collective_id=1, has_side_effects=True),
    )(pack)
    return gathered.reshape(n * rows, width)


def f32dot(a, b):
    return jnp.dot(a, b, preferred_element_type=jnp.float32)


def layer_kernel(
    n_sp, n_local, resid, hs, hl, gain, wts, wos, wol, wg_h, wu_h, wd_h, sg_h, su_h, sd_h,
    out_ref,
    wg, wu, wd, sg, su, sd, part, pc, psx, px, blk, stream, gath, acc, ybuf, rc, sx, rx, sz, rz, own,
    wsem, psend, precv, zsend, xsend, csend, grecv, ycs, ycr, yxs, yxr, yzs, yzr,
):
    s = lax.axis_index("sp")
    t = lax.axis_index("tp")
    rows, width = resid.shape
    xp = lax.rem(t + 2, 4)
    cp = t + 1 - 2 * lax.rem(t, 2)
    cxp = lax.rem(cp + 2, 4)
    peers = [{"sp": lax.rem(s + k, n_sp)} for k in range(1, n_sp)] + [{"tp": xp}, {"tp": cp}]
    loads = [
        pltpu.make_async_copy(src, dst, wsem.at[i])
        for i, (src, dst) in enumerate(
            ((sg_h, sg), (su_h, su), (sd_h, sd), (wg_h, wg), (wu_h, wu), (wd_h, wd))
        )
    ]
    greet(peers)
    for load in loads:
        load.start()

    def strip(index):
        return pl.ds(pl.multiple_of(index * rows, rows), rows)

    part[...] = (f32dot(hs[...], wos[...]) + f32dot(hl[...], wol[...])).astype(jnp.bfloat16)
    to_x = remote(part.at[strip(cxp)], pc.at[1], psend.at[0], precv.at[0], {"tp": cp})
    to_own = remote(part.at[strip(cp)], pc.at[0], psend.at[1], precv.at[1], {"tp": cp})
    to_x.start()
    to_own.start()
    to_x.wait_recv()
    psx[...] = (part[strip(xp)].astype(jnp.float32) + pc[1].astype(jnp.float32)).astype(jnp.bfloat16)
    across = remote(psx, px, psend.at[2], precv.at[2], {"tp": xp})
    across.start()
    to_own.wait_recv()
    across.wait_recv()
    head_sum = part[strip(t)].astype(jnp.float32) + pc[0].astype(jnp.float32) + px[...].astype(jnp.float32)
    summed = (resid[...].astype(jnp.float32) + head_sum).astype(jnp.bfloat16)
    stream[...] = summed
    wide = summed.astype(jnp.float32)
    scale = lax.rsqrt(jnp.mean(wide * wide, axis=-1, keepdims=True) + norm_eps)
    blk[:, :width] = (wide * scale * gain[...]).astype(jnp.bfloat16)
    blk[:, width:] = wts[...]

    mine = gath.at[s, strip(t)]
    z_out = [
        remote(blk, mine, zsend.at[k], grecv.at[s, t], {"sp": lax.rem(s + k + 1, n_sp)})
        for k in range(n_sp - 1)
    ]
    x_own = remote(blk, mine, xsend.at[0], grecv.at[s, t], {"tp": xp})
    c_own = remote(blk, mine, csend.at[0, 0], grecv.at[s, t], {"tp": cp})
    x_own.start()
    for copy in z_out:
        copy.start()
    c_own.start()
    gath[s, strip(t)] = blk[...]
    for load in loads:
        load.wait()

    def block_of(k, column):
        row = lax.rem(s - k + n_sp, n_sp)
        return gath.at[row, strip(column)], grecv.at[row, column]

    def pass_on(k, column, send, peer):
        ref, sem = block_of(k, column)
        return remote(ref, ref, send, sem, peer)

    def core_part(k, slot):
        index = cp if slot == 0 else cxp
        return remote(ybuf.at[k, strip(index)], rc.at[k, slot], ycs.at[k, slot], ycr.at[k, slot], {"tp": cp})

    def x_part(k):
        return remote(sx.at[k], rx.at[k], yxs.at[k], yxr.at[k], {"tp": xp})

    def z_part(k):
        return remote(sz.at[k], rz.at[k], yzs.at[k], yzr.at[k], {"sp": lax.rem(s - k + n_sp, n_sp)})

    @pl.loop(0, n_sp + 2)
    def _(k):
        @pl.when(k < n_sp - 1)
        def _():
            ahead = pass_on(k + 1, t, xsend.at[k + 1], {"tp": xp})
            ahead.wait_recv()
            ahead.start()
            pass_on(k + 1, t, csend.at[k + 1, 0], {"tp": cp}).start()

        @pl.when(k < n_sp)
        def _():
            over = pass_on(k, xp, csend.at[k, 1], {"tp": cp})
            over.wait_recv()
            over.start()
            pass_on(k, cp, csend.at[k, 0], {"tp": cp}).wait_recv()
            pass_on(k, cxp, csend.at[k, 1], {"tp": cp}).wait_recv()
            row = lax.rem(s - k + n_sp, n_sp)
            tokens = gath[row, :, :width]
            marks = gath[row, :, width:].astype(jnp.float32)
            lane = lax.broadcasted_iota(jnp.int32, marks.shape, 1)

            @pl.when(k == 0)
            def _():
                gate = f32dot(tokens, sg[...])
                hidden = (gate / (1.0 + jnp.exp(-gate)) * f32dot(tokens, su[...])).astype(jnp.bfloat16)
                acc[...] = f32dot(hidden, sd[...])

            @pl.when(k > 0)
            def _():
                acc[...] = jnp.zeros_like(acc)

            experts = n_local * n_sp
            for e in range(n_local):
                number = s * n_local + e
                hit = (lane == number) | (lane == number + experts) | (lane == number + 2 * experts)
                weight = jnp.sum(jnp.where(hit, marks, 0.0), axis=1, keepdims=True)
                gate = f32dot(tokens, wg[e])
                hidden = (gate / (1.0 + jnp.exp(-gate)) * f32dot(tokens, wu[e])).astype(jnp.bfloat16)
                acc[...] += weight * f32dot(hidden, wd[e])
            ybuf[k] = acc[...].astype(jnp.bfloat16)
            core_part(k, 1).start()
            core_part(k, 0).start()

        @pl.when((k >= 1) & (k <= n_sp))
        def _():
            j = k - 1
            core_part(j, 1).wait_recv()
            sx[j] = (ybuf[j, strip(xp)].astype(jnp.float32) + rc[j, 1].astype(jnp.float32)).astype(jnp.bfloat16)
            x_part(j).start()

        @pl.when(k >= 2)
        def _():
            j = k - 2
            core_part(j, 0).wait_recv()
            x_part(j).wait_recv()
            total = ybuf[j, strip(t)].astype(jnp.float32) + rc[j, 0].astype(jnp.float32) + rx[j].astype(jnp.float32)

            @pl.when(j > 0)
            def _():
                sz[j] = total.astype(jnp.bfloat16)
                z_part(j).start()

            @pl.when(j == 0)
            def _():
                own[...] = total

    result = stream[...].astype(jnp.float32) + own[...]
    for k in range(1, n_sp):
        z_part(k).wait_recv()
        result = result + rz[k].astype(jnp.float32)
    out_ref[...] = result.astype(jnp.bfloat16)

    to_x.wait_send()
    to_own.wait_send()
    across.wait_send()
    x_own.wait_send()
    c_own.wait_send()
    for copy in z_out:
        copy.wait_send()
    for k in range(n_sp):
        if k > 0:
            pass_on(k, t, xsend.at[k], {"tp": xp}).wait_send()
            pass_on(k, t, csend.at[k, 0], {"tp": cp}).wait_send()
            z_part(k).wait_send()
        pass_on(k, xp, csend.at[k, 1], {"tp": cp}).wait_send()
        core_part(k, 0).wait_send()
        core_part(k, 1).wait_send()
        x_part(k).wait_send()


def layer_call(resid, hs, hl, gain, wts, wos, wol, wg, wu, wd, sg, su, sd):
    n_sp = lax.axis_size("sp")
    n_tp = lax.axis_size("tp")
    rows, width = resid.shape
    n_local = wg.shape[0]
    padded = width + wts.shape[1]
    bf, f32 = jnp.bfloat16, jnp.float32
    dma = pltpu.SemaphoreType.DMA
    vmem = pl.BlockSpec(memory_space=pltpu.VMEM)
    anywhere = pl.BlockSpec(memory_space=pl.ANY)
    scratch = [pltpu.VMEM(w.shape, w.dtype) for w in (wg, wu, wd, sg, su, sd)] + [
        pltpu.VMEM((n_tp * rows, width), bf),
        pltpu.VMEM((2, rows, width), bf),
        pltpu.VMEM((rows, width), bf),
        pltpu.VMEM((rows, width), bf),
        pltpu.VMEM((rows, padded), bf),
        pltpu.VMEM((rows, width), bf),
        pltpu.VMEM((n_sp, n_tp * rows, padded), bf),
        pltpu.VMEM((n_tp * rows, width), f32),
        pltpu.VMEM((n_sp, n_tp * rows, width), bf),
        pltpu.VMEM((n_sp, 2, rows, width), bf),
        pltpu.VMEM((n_sp, rows, width), bf),
        pltpu.VMEM((n_sp, rows, width), bf),
        pltpu.VMEM((n_sp, rows, width), bf),
        pltpu.VMEM((n_sp, rows, width), bf),
        pltpu.VMEM((rows, width), f32),
        dma((6,)), dma((3,)), dma((3,)),
        dma((n_sp - 1,)), dma((n_sp,)), dma((n_sp, 2)), dma((n_sp, n_tp)),
        dma((n_sp, 2)), dma((n_sp, 2)), dma((n_sp,)), dma((n_sp,)), dma((n_sp,)), dma((n_sp,)),
    ]
    return pl.pallas_call(
        functools.partial(layer_kernel, n_sp, n_local),
        out_shape=jax.ShapeDtypeStruct((rows, width), bf),
        in_specs=[vmem] * 7 + [anywhere] * 6,
        out_specs=vmem,
        scratch_shapes=scratch,
        compiler_params=pltpu.CompilerParams(
            collective_id=2, has_side_effects=True, vmem_limit_bytes=48 * 1024 * 1024
        ),
    )(resid, hs, hl, gain, wts, wos, wol, wg, wu, wd, sg, su, sd)


def attend(queries, keys, values):
    rows, heads, group, channels = queries.shape
    keys = keys.reshape(keys.shape[0], heads, channels)
    values = values.reshape(values.shape[0], heads, channels)
    scores = jnp.einsum("qkgd,skd->kgqs", queries, keys, preferred_element_type=jnp.float32) * channels ** (-0.5)
    raised = jnp.exp(scores - jnp.max(scores, axis=-1, keepdims=True))
    totals = jnp.sum(raised, axis=-1)
    mixture = jnp.einsum(
        "kgqs,skd->qkgd", raised.astype(jnp.bfloat16), values, preferred_element_type=jnp.float32
    )
    mixture = mixture / jnp.transpose(totals, (2, 0, 1))[..., None]
    return mixture.reshape(rows, -1).astype(jnp.bfloat16)


def dense_local(
    residual_in, q_small, k_small, v_small, q_large, k_large, v_large,
    gain_qs, gain_ks, gain_ql, gain_kl, w_out_small, w_out_large, g_ffn,
    routes, route_w, w_gate, w_up, w_down, ws_gate, ws_up, ws_down,
):
    local_rows = q_small.shape[0]
    positions = lax.axis_index("sp") * local_rows + jnp.arange(local_rows, dtype=jnp.int32)
    key_small = norm_rotate(k_small, gain_ks, positions, GRID_W)
    key_large = norm_rotate(k_large, gain_kl, positions, GRID_W)
    kv_small, kv_large = key_small.shape[1], key_large.shape[1]
    pack = jnp.concatenate(
        [key_small.reshape(local_rows, -1), v_small, key_large.reshape(local_rows, -1), v_large], axis=1
    )
    gathered = gather_rows(pack)
    query_small = norm_rotate(q_small, gain_qs, positions, GRID_W)
    query_large = norm_rotate(q_large, gain_ql, positions, GRID_W)
    query_small = query_small.reshape(local_rows, kv_small, -1, gain_qs.shape[0])
    query_large = query_large.reshape(local_rows, kv_large, -1, gain_ql.shape[0])
    a, b = k_small.shape[1], k_large.shape[1]
    heads_small = attend(query_small, gathered[:, :a], gathered[:, a : 2 * a])
    heads_large = attend(query_large, gathered[:, 2 * a : 2 * a + b], gathered[:, 2 * a + b :])
    experts = w_gate.shape[0] * lax.axis_size("sp")
    named = routes[:, :, None] == jnp.arange(experts, dtype=jnp.int32)
    marks = jnp.sum(jnp.where(named, route_w[:, :, None], 0.0), axis=1)
    first = lax.reduce_precision(marks, 8, 7)
    second = lax.reduce_precision(marks - first, 8, 7)
    third = marks - first - second
    marks = jnp.concatenate([first, second, third], axis=1)
    marks = jnp.pad(marks, ((0, 0), (0, 128 - marks.shape[1]))).astype(jnp.bfloat16)
    return layer_call(
        residual_in, heads_small, heads_large, g_ffn[None, :], marks, w_out_small, w_out_large,
        w_gate, w_up, w_down, ws_gate, ws_up, ws_down,
    )


def fits_dense(mesh, *arrays):
    routes, w_gate = arrays[14], arrays[16]
    ways = mesh.shape["sp"] * mesh.shape["tp"]
    rows_dev = routes.shape[0] // (ways * mesh.shape["grp"])
    experts = w_gate.shape[0]
    capacity = max(2, 2 * rows_dev * TOPK // experts)
    return mesh.shape["tp"] == 4 and capacity >= rows_dev and 3 * experts <= 128


def solution(mesh):
    placed = (
        P(("grp", "sp", "tp"), None),
        P(("grp", "sp"), "tp"),
        P(("grp", "sp"), "tp"),
        P(("grp", "sp"), "tp"),
        P(("grp", "sp"), "tp"),
        P(("grp", "sp"), "tp"),
        P(("grp", "sp"), "tp"),
        P(),
        P(),
        P(),
        P(),
        P("tp", None),
        P("tp", None),
        P(),
        P(("grp", "sp", "tp"), None),
        P(("grp", "sp", "tp"), None),
        P("sp", None, "tp"),
        P("sp", None, "tp"),
        P("sp", "tp", None),
        P(None, "tp"),
        P(None, "tp"),
        P("tp", None),
    )

    def whole(*arrays):
        body = dense_local if fits_dense(mesh, *arrays) else local
        return jax.shard_map(
            body, mesh=mesh, in_specs=placed, out_specs=P(("grp", "sp", "tp"), None), check_vma=False
        )(*arrays)

    return whole
```

```python
import functools
import math

import jax
import jax.numpy as jnp
from jax import lax
from jax.experimental import pallas as pl
from jax.experimental.pallas import tpu as pltpu
from jax.sharding import PartitionSpec as P

GRID_W = 64
TOPK = 4


norm_eps = 1e-06
rope_base = 10000.0
far_below = -1e30


def rotate_pairs(values, angles):
    front_half, back_half = jnp.split(values, 2, axis=-1)
    cosine_vals = jnp.cos(angles)[:, None, :]
    sine_vals = jnp.sin(angles)[:, None, :]
    return jnp.concatenate(
        [
            front_half * cosine_vals - back_half * sine_vals,
            front_half * sine_vals + back_half * cosine_vals,
        ],
        axis=-1,
    )


def norm_rotate(heads_in, gain, positions, grid_width):
    channels = gain.shape[0]
    values = heads_in.astype(jnp.float32).reshape(heads_in.shape[0], -1, channels)
    values = values * lax.rsqrt(jnp.mean(values * values, axis=-1, keepdims=True) + norm_eps) * gain
    quarter = channels // 4
    inverse = 1.0 / rope_base ** (jnp.arange(quarter, dtype=jnp.float32) / quarter)
    grid_rows = (positions // grid_width).astype(jnp.float32)
    grid_cols = (positions % grid_width).astype(jnp.float32)
    half_width = channels // 2
    turned = jnp.concatenate(
        [
            rotate_pairs(values[..., :half_width], grid_rows[:, None] * inverse[None, :]),
            rotate_pairs(values[..., half_width:], grid_cols[:, None] * inverse[None, :]),
        ],
        axis=-1,
    )
    return turned.astype(jnp.bfloat16)


def absorb(carried, segment, queries):
    peak_val, totals, mixture = carried
    kv_heads = queries.shape[1]
    channels = queries.shape[3]
    pairs = segment.reshape(segment.shape[0], 2, kv_heads, channels)
    scores = jnp.einsum(
        "qkgd,skd->kgqs", queries, pairs[:, 0], preferred_element_type=jnp.float32
    ) * channels ** (-0.5)
    new_peak = jnp.maximum(peak_val, jnp.max(scores, axis=-1))
    weights_raw = jnp.exp(scores - new_peak[..., None])
    shrink = jnp.exp(peak_val - new_peak)
    totals = totals * shrink + jnp.sum(weights_raw, axis=-1)
    update = jnp.einsum(
        "kgqs,skd->qkgd",
        weights_raw.astype(jnp.bfloat16),
        pairs[:, 1],
        preferred_element_type=jnp.float32,
    )
    mixture = mixture * jnp.transpose(shrink, (2, 0, 1))[..., None] + update
    return (new_peak, totals, mixture)


def absorb_blocks(carried, segment, queries):
    row_count = segment.shape[0]
    block_rows = math.gcd(row_count, 1024)
    stacked = segment.reshape(row_count // block_rows, block_rows, segment.shape[1])

    def fold_step(inner, key_block):
        return (absorb(inner, key_block, queries), None)

    carried, _ = lax.scan(fold_step, carried, stacked)
    return carried


def start_state(queries):
    local_rows, kv_heads, group, channels = queries.shape
    return (
        jnp.full((kv_heads, group, local_rows), far_below, jnp.float32),
        jnp.zeros((kv_heads, group, local_rows), jnp.float32),
        jnp.zeros(queries.shape, jnp.float32),
    )


def finish(carried):
    peak_val, totals, mixture = carried
    heads_out = mixture / jnp.transpose(totals, (2, 0, 1))[..., None]
    return heads_out.reshape(heads_out.shape[0], -1).astype(jnp.bfloat16)


def local(
    residual_in,
    q_small,
    k_small,
    v_small,
    q_large,
    k_large,
    v_large,
    gain_qs,
    gain_ks,
    gain_ql,
    gain_kl,
    w_out_small,
    w_out_large,
    g_ffn,
    routes,
    route_w,
    w_gate,
    w_up,
    w_down,
    ws_gate,
    ws_up,
    ws_down,
):
    local_rows = q_small.shape[0]
    positions = lax.axis_index("sp") * local_rows + jnp.arange(local_rows, dtype=jnp.int32)
    query_small = norm_rotate(q_small, gain_qs, positions, GRID_W)
    key_small = norm_rotate(k_small, gain_ks, positions, GRID_W)
    query_large = norm_rotate(q_large, gain_ql, positions, GRID_W)
    key_large = norm_rotate(k_large, gain_kl, positions, GRID_W)
    query_small = query_small.reshape(local_rows, key_small.shape[1], -1, gain_qs.shape[0])
    query_large = query_large.reshape(local_rows, key_large.shape[1], -1, gain_ql.shape[0])
    pack_small = jnp.concatenate([key_small.reshape(local_rows, -1), v_small], axis=1)
    pack_large = jnp.concatenate([key_large.reshape(local_rows, -1), v_large], axis=1)
    segment = (
        lax.all_gather(pack_small, "sp", axis=0, tiled=True),
        lax.all_gather(pack_large, "sp", axis=0, tiled=True),
    )
    heads_small = finish(absorb_blocks(start_state(query_small), segment[0], query_small))
    heads_large = finish(absorb_blocks(start_state(query_large), segment[1], query_large))
    tp_count = lax.axis_size("tp")
    sp_count = lax.axis_size("sp")
    rows_dev = local_rows // tp_count
    head_sum = lax.psum_scatter(
        (
            jnp.dot(heads_small, w_out_small, preferred_element_type=jnp.float32)
            + jnp.dot(heads_large, w_out_large, preferred_element_type=jnp.float32)
        ).astype(jnp.bfloat16),
        "tp",
        scatter_dimension=0,
        tiled=True,
    ).astype(jnp.float32)
    stream = (residual_in.astype(jnp.float32) + head_sum).astype(jnp.bfloat16)
    stream32 = lax.optimization_barrier(stream).astype(jnp.float32)
    normed = (
        stream32
        * lax.rsqrt(jnp.mean(stream32 * stream32, axis=-1, keepdims=True) + norm_eps)
        * g_ffn
    ).astype(jnp.bfloat16)
    channels = normed.shape[1]
    segment = lax.all_gather(normed, "tp", axis=0, tiled=True)
    gate_act = jnp.dot(segment, ws_gate, preferred_element_type=jnp.float32)
    up_act = jnp.dot(segment, ws_up, preferred_element_type=jnp.float32)
    hidden_shared = (jax.nn.silu(gate_act) * up_act).astype(jnp.bfloat16)
    shared = lax.psum_scatter(
        jnp.dot(hidden_shared, ws_down, preferred_element_type=jnp.float32).astype(jnp.bfloat16),
        "tp",
        scatter_dimension=0,
        tiled=True,
    ).astype(jnp.float32)
    local_experts = w_gate.shape[0]
    experts = local_experts * sp_count
    capacity = max(2, 2 * rows_dev * TOPK // experts)
    flat_ids = routes.reshape(-1)
    one_hot = (flat_ids[:, None] == jnp.arange(experts, dtype=jnp.int32)[None, :]).astype(jnp.int32)
    slot_ids = jnp.sum((jnp.cumsum(one_hot, axis=0) - 1) * one_hot, axis=1)
    targets = flat_ids * capacity + slot_ids
    owners = jnp.arange(rows_dev * TOPK, dtype=jnp.int32) // TOPK
    outbox = jnp.zeros((experts * capacity, channels), jnp.bfloat16).at[targets].set(normed[owners])
    arrived = lax.all_to_all(outbox, "sp", split_axis=0, concat_axis=0, tiled=True)
    arrived = lax.all_gather(
        arrived.reshape(sp_count, 1, local_experts, capacity, channels), "tp", axis=1, tiled=True
    )
    gate_act = jnp.einsum("abecd,edf->abecf", arrived, w_gate, preferred_element_type=jnp.float32)
    up_act = jnp.einsum("abecd,edf->abecf", arrived, w_up, preferred_element_type=jnp.float32)
    hidden = (jax.nn.silu(gate_act) * up_act).astype(jnp.bfloat16)
    partial_value = jnp.einsum(
        "abecf,efd->abecd", hidden, w_down, preferred_element_type=jnp.float32
    )
    summed = lax.psum_scatter(
        partial_value.astype(jnp.bfloat16), "tp", scatter_dimension=1, tiled=True
    )
    returned = lax.all_to_all(
        summed.reshape(sp_count * local_experts * capacity, channels),
        "sp",
        split_axis=0,
        concat_axis=0,
        tiled=True,
    )
    picked = returned[targets].reshape(rows_dev, TOPK, channels).astype(jnp.float32)
    routed = jnp.sum(picked * route_w[..., None], axis=1)
    return (stream32 + routed + shared).astype(jnp.bfloat16)


MESH = pl.DeviceIdType.MESH


def greet(peers):
    barrier = pltpu.get_barrier_semaphore()
    for peer in peers:
        pl.semaphore_signal(barrier, inc=1, device_id=peer, device_id_type=MESH)
    pl.semaphore_wait(barrier, len(peers))


def remote(src, dst, send, recv, peer):
    return pltpu.make_async_remote_copy(
        src_ref=src, dst_ref=dst, send_sem=send, recv_sem=recv, device_id=peer, device_id_type=MESH
    )


def f32dot(a, b):
    return jnp.dot(a, b, preferred_element_type=jnp.float32)


def rotated(tile, turn_c, turn_s, channels):
    lanes = tile.shape[1]
    row = lax.broadcasted_iota(jnp.int32, (lanes, lanes), 0)
    column = lax.broadcasted_iota(jnp.int32, (lanes, lanes), 1)
    swap = jnp.where((row ^ column) == channels // 4, 1.0, 0.0).astype(jnp.bfloat16)
    same = jnp.where((row ^ column) < channels, 1.0, 0.0).astype(jnp.bfloat16)
    wide = tile.astype(jnp.float32)
    square = wide * wide
    upper = square.astype(jnp.bfloat16)
    lower = (square - upper.astype(jnp.float32)).astype(jnp.bfloat16)
    mean = (f32dot(upper, same) + f32dot(lower, same)) * (1.0 / channels)
    return lax.rsqrt(mean + norm_eps) * (wide * turn_c + f32dot(tile, swap) * turn_s)


def attention(
    s, n_sp, small, large, heads_in, v_large, turn_c, turn_s,
    kv_own, kv, q_s, q_l, p_s, p_l, hs, hl, kvr, kup, kdown,
):
    rows = heads_in.shape[0]
    n_small, n_large = q_s.shape[0] // rows, q_l.shape[0] // rows

    def turned(start, channels):
        lanes = pl.ds(start, 128)
        return rotated(heads_in[:, lanes], turn_c[:, lanes], turn_s[:, lanes], channels)

    first = n_small * small
    mixed = turned(first, small)
    lane = lax.broadcasted_iota(jnp.int32, mixed.shape, 1)
    plain = heads_in[:, pl.ds(first, 128)].astype(jnp.float32)
    kv_own[:, 0:128] = jnp.where(lane < small, mixed, plain).astype(jnp.bfloat16)
    kv_own[:, 128:256] = turned(first + 128 + n_large * large, large).astype(jnp.bfloat16)
    kv_own[:, 256:384] = v_large[...]

    def send(source, row, sems, step, target):
        return pltpu.make_async_remote_copy(
            src_ref=source, dst_ref=kv.at[row], send_sem=sems.at[step], recv_sem=kvr.at[row],
            device_id={"sp": lax.rem(target + n_sp, n_sp)}, device_id_type=MESH,
        )

    @pl.when(s < n_sp - 1)
    def _():
        send(kv_own, s, kup, 0, s + 1).start()

    @pl.when(s > 0)
    def _():
        send(kv_own, s, kdown, 0, s - 1).start()

    kv[s] = kv_own[...]
    for tile in range(n_small * small // 128):
        both = turned(tile * 128, small).astype(jnp.bfloat16)
        for half in range(128 // small):
            q_s[pl.ds((tile * (128 // small) + half) * rows, rows), :] = both[:, half * small : (half + 1) * small]
    for tile in range(n_large):
        q_l[pl.ds(tile * rows, rows), :] = turned(first + 128 + tile * 128, large).astype(jnp.bfloat16)

    def score(row):
        span = pl.ds(pl.multiple_of(row * rows, rows), rows)
        keys = kv[row, :, 0:small]
        p_s[:, span] = lax.dot_general(
            q_s[...], keys, (((1,), (1,)), ((), ())), preferred_element_type=jnp.float32
        ) * small ** (-0.5)
        keys = kv[row, :, 128:256]
        p_l[:, span] = lax.dot_general(
            q_l[...], keys, (((1,), (1,)), ((), ())), preferred_element_type=jnp.float32
        ) * large ** (-0.5)

    score(s)

    @pl.loop(1, n_sp)
    def _(d):
        below, above = s - d, s + d

        @pl.when(below >= 0)
        def _():
            send(kv.at[below], below, kup, d, s + 1).wait_recv()

            @pl.when(s < n_sp - 1)
            def _():
                send(kv.at[below], below, kup, d, s + 1).start()

        @pl.when(above < n_sp)
        def _():
            send(kv.at[above], above, kdown, d, s - 1).wait_recv()

            @pl.when(s > 0)
            def _():
                send(kv.at[above], above, kdown, d, s - 1).start()

        @pl.when(below >= 0)
        def _():
            score(below)

        @pl.when(above < n_sp)
        def _():
            score(above)

    def head(index, scores, low, width, out):
        block = scores[pl.ds(index * rows, rows), :]
        raised = jnp.exp(block - jnp.max(block, axis=-1, keepdims=True))
        total = jnp.sum(raised, axis=-1, keepdims=True)
        weights = raised.astype(jnp.bfloat16)
        mixture = f32dot(weights[:, :rows], kv[0, :, low : low + width])
        for row in range(1, n_sp):
            mixture += f32dot(weights[:, row * rows : (row + 1) * rows], kv[row, :, low : low + width])
        out[:, index * width : (index + 1) * width] = (mixture / total).astype(jnp.bfloat16)

    for index in range(n_small):
        head(index, p_s, small, small, hs)
    for index in range(n_large):
        head(index, p_l, 256, large, hl)

    @pl.loop(0, n_sp)
    def _(d):
        @pl.when((s < n_sp - 1) & (s - d >= 0))
        def _():
            send(kv_own, s, kup, d, s + 1).wait_send()

        @pl.when((s > 0) & (s + d < n_sp))
        def _():
            send(kv_own, s, kdown, d, s - 1).wait_send()


def layer_kernel(
    n_sp, n_local, small, large, resid, heads_in, v_large, turn_c, turn_s, gain, wts, wos_h, wol_h, wg_h, wu_h, wd_h, sg_h, su_h, sd_h,
    out_ref,
    wos, wol, wg, wu, wd, sg, su, sd, kv_own, kv, q_s, q_l, p_s, p_l, hs, hl, part, pc, psx, px, blk, stream, gath, acc, ybuf, rc, sx, rx, sz, rz, own,
    wsem, kvr, kup, kdown, psend, precv, zsend, xsend, csend, grecv, ycs, ycr, yxs, yxr, yzs, yzr,
):
    s = lax.axis_index("sp")
    t = lax.axis_index("tp")
    rows, width = resid.shape
    xp = lax.rem(t + 2, 4)
    cp = t + 1 - 2 * lax.rem(t, 2)
    cxp = lax.rem(cp + 2, 4)
    peers = [{"sp": lax.rem(s + k, n_sp)} for k in range(1, n_sp)] + [{"tp": xp}, {"tp": cp}]
    loads = [
        pltpu.make_async_copy(src, dst, wsem.at[i])
        for i, (src, dst) in enumerate(
            ((wos_h, wos), (wol_h, wol), (sg_h, sg), (su_h, su), (sd_h, sd), (wg_h, wg), (wu_h, wu), (wd_h, wd))
        )
    ]
    greet(peers)
    for load in loads:
        load.start()

    def strip(index):
        return pl.ds(pl.multiple_of(index * rows, rows), rows)

    attention(
        s, n_sp, small, large, heads_in, v_large, turn_c, turn_s,
        kv_own, kv, q_s, q_l, p_s, p_l, hs, hl, kvr, kup, kdown,
    )
    loads[0].wait()
    loads[1].wait()
    part[...] = (f32dot(hs[...], wos[...]) + f32dot(hl[...], wol[...])).astype(jnp.bfloat16)
    to_x = remote(part.at[strip(cxp)], pc.at[1], psend.at[0], precv.at[0], {"tp": cp})
    to_own = remote(part.at[strip(cp)], pc.at[0], psend.at[1], precv.at[1], {"tp": cp})
    to_x.start()
    to_own.start()
    to_x.wait_recv()
    psx[...] = (part[strip(xp)].astype(jnp.float32) + pc[1].astype(jnp.float32)).astype(jnp.bfloat16)
    across = remote(psx, px, psend.at[2], precv.at[2], {"tp": xp})
    across.start()
    to_own.wait_recv()
    across.wait_recv()
    head_sum = part[strip(t)].astype(jnp.float32) + pc[0].astype(jnp.float32) + px[...].astype(jnp.float32)
    summed = (resid[...].astype(jnp.float32) + head_sum).astype(jnp.bfloat16)
    stream[...] = summed
    wide = summed.astype(jnp.float32)
    scale = lax.rsqrt(jnp.mean(wide * wide, axis=-1, keepdims=True) + norm_eps)
    blk[:, :width] = (wide * scale * gain[...]).astype(jnp.bfloat16)
    blk[:, width:] = wts[...]

    mine = gath.at[s, strip(t)]
    z_out = [
        remote(blk, mine, zsend.at[k], grecv.at[s, t], {"sp": lax.rem(s + k + 1, n_sp)})
        for k in range(n_sp - 1)
    ]
    x_own = remote(blk, mine, xsend.at[0], grecv.at[s, t], {"tp": xp})
    c_own = remote(blk, mine, csend.at[0, 0], grecv.at[s, t], {"tp": cp})
    x_own.start()
    for copy in z_out:
        copy.start()
    c_own.start()
    gath[s, strip(t)] = blk[...]
    for load in loads[2:]:
        load.wait()

    def block_of(k, column):
        row = lax.rem(s - k + n_sp, n_sp)
        return gath.at[row, strip(column)], grecv.at[row, column]

    def pass_on(k, column, send, peer):
        ref, sem = block_of(k, column)
        return remote(ref, ref, send, sem, peer)

    def core_part(k, slot):
        index = cp if slot == 0 else cxp
        return remote(ybuf.at[k, strip(index)], rc.at[k, slot], ycs.at[k, slot], ycr.at[k, slot], {"tp": cp})

    def x_part(k):
        return remote(sx.at[k], rx.at[k], yxs.at[k], yxr.at[k], {"tp": xp})

    def z_part(k):
        return remote(sz.at[k], rz.at[k], yzs.at[k], yzr.at[k], {"sp": lax.rem(s - k + n_sp, n_sp)})

    @pl.loop(0, n_sp + 2)
    def _(k):
        @pl.when(k < n_sp - 1)
        def _():
            ahead = pass_on(k + 1, t, xsend.at[k + 1], {"tp": xp})
            ahead.wait_recv()
            ahead.start()
            pass_on(k + 1, t, csend.at[k + 1, 0], {"tp": cp}).start()

        @pl.when(k < n_sp)
        def _():
            over = pass_on(k, xp, csend.at[k, 1], {"tp": cp})
            over.wait_recv()
            over.start()
            pass_on(k, cp, csend.at[k, 0], {"tp": cp}).wait_recv()
            pass_on(k, cxp, csend.at[k, 1], {"tp": cp}).wait_recv()
            row = lax.rem(s - k + n_sp, n_sp)
            tokens = gath[row, :, :width]
            marks = gath[row, :, width:].astype(jnp.float32)
            lane = lax.broadcasted_iota(jnp.int32, marks.shape, 1)

            @pl.when(k == 0)
            def _():
                gate = f32dot(tokens, sg[...])
                hidden = (gate / (1.0 + jnp.exp(-gate)) * f32dot(tokens, su[...])).astype(jnp.bfloat16)
                acc[...] = f32dot(hidden, sd[...])

            @pl.when(k > 0)
            def _():
                acc[...] = jnp.zeros_like(acc)

            experts = n_local * n_sp
            for e in range(n_local):
                number = s * n_local + e
                hit = (lane == number) | (lane == number + experts) | (lane == number + 2 * experts)
                weight = jnp.sum(jnp.where(hit, marks, 0.0), axis=1, keepdims=True)
                gate = f32dot(tokens, wg[e])
                hidden = (gate / (1.0 + jnp.exp(-gate)) * f32dot(tokens, wu[e])).astype(jnp.bfloat16)
                acc[...] += weight * f32dot(hidden, wd[e])
            ybuf[k] = acc[...].astype(jnp.bfloat16)
            core_part(k, 1).start()
            core_part(k, 0).start()

        @pl.when((k >= 1) & (k <= n_sp))
        def _():
            j = k - 1
            core_part(j, 1).wait_recv()
            sx[j] = (ybuf[j, strip(xp)].astype(jnp.float32) + rc[j, 1].astype(jnp.float32)).astype(jnp.bfloat16)
            x_part(j).start()

        @pl.when(k >= 2)
        def _():
            j = k - 2
            core_part(j, 0).wait_recv()
            x_part(j).wait_recv()
            total = ybuf[j, strip(t)].astype(jnp.float32) + rc[j, 0].astype(jnp.float32) + rx[j].astype(jnp.float32)

            @pl.when(j > 0)
            def _():
                sz[j] = total.astype(jnp.bfloat16)
                z_part(j).start()

            @pl.when(j == 0)
            def _():
                own[...] = total

    result = stream[...].astype(jnp.float32) + own[...]
    for k in range(1, n_sp):
        z_part(k).wait_recv()
        result = result + rz[k].astype(jnp.float32)
    out_ref[...] = result.astype(jnp.bfloat16)

    to_x.wait_send()
    to_own.wait_send()
    across.wait_send()
    x_own.wait_send()
    c_own.wait_send()
    for copy in z_out:
        copy.wait_send()
    for k in range(n_sp):
        if k > 0:
            pass_on(k, t, xsend.at[k], {"tp": xp}).wait_send()
            pass_on(k, t, csend.at[k, 0], {"tp": cp}).wait_send()
            z_part(k).wait_send()
        pass_on(k, xp, csend.at[k, 1], {"tp": cp}).wait_send()
        core_part(k, 0).wait_send()
        core_part(k, 1).wait_send()
        x_part(k).wait_send()


def layer_call(small, large, resid, heads_in, v_large, turn_c, turn_s, gain, wts, wos, wol, wg, wu, wd, sg, su, sd):
    n_sp = lax.axis_size("sp")
    n_tp = lax.axis_size("tp")
    rows, width = resid.shape
    n_local = wg.shape[0]
    block = n_tp * rows
    padded = width + wts.shape[1]
    bf, f32 = jnp.bfloat16, jnp.float32
    dma = pltpu.SemaphoreType.DMA
    vmem = pl.BlockSpec(memory_space=pltpu.VMEM)
    anywhere = pl.BlockSpec(memory_space=pl.ANY)
    scratch = [pltpu.VMEM(w.shape, w.dtype) for w in (wos, wol, wg, wu, wd, sg, su, sd)] + [
        pltpu.VMEM((block, 384), bf),
        pltpu.VMEM((n_sp, block, 384), bf),
        pltpu.VMEM((wos.shape[0] // small * block, small), bf),
        pltpu.VMEM((wol.shape[0] // large * block, large), bf),
        pltpu.VMEM((wos.shape[0] // small * block, n_sp * block), f32),
        pltpu.VMEM((wol.shape[0] // large * block, n_sp * block), f32),
        pltpu.VMEM((block, wos.shape[0]), bf),
        pltpu.VMEM((block, wol.shape[0]), bf),
        pltpu.VMEM((n_tp * rows, width), bf),
        pltpu.VMEM((2, rows, width), bf),
        pltpu.VMEM((rows, width), bf),
        pltpu.VMEM((rows, width), bf),
        pltpu.VMEM((rows, padded), bf),
        pltpu.VMEM((rows, width), bf),
        pltpu.VMEM((n_sp, n_tp * rows, padded), bf),
        pltpu.VMEM((n_tp * rows, width), f32),
        pltpu.VMEM((n_sp, n_tp * rows, width), bf),
        pltpu.VMEM((n_sp, 2, rows, width), bf),
        pltpu.VMEM((n_sp, rows, width), bf),
        pltpu.VMEM((n_sp, rows, width), bf),
        pltpu.VMEM((n_sp, rows, width), bf),
        pltpu.VMEM((n_sp, rows, width), bf),
        pltpu.VMEM((rows, width), f32),
        dma((8,)), dma((n_sp,)), dma((n_sp,)), dma((n_sp,)), dma((3,)), dma((3,)),
        dma((n_sp - 1,)), dma((n_sp,)), dma((n_sp, 2)), dma((n_sp, n_tp)),
        dma((n_sp, 2)), dma((n_sp, 2)), dma((n_sp,)), dma((n_sp,)), dma((n_sp,)), dma((n_sp,)),
    ]
    return pl.pallas_call(
        functools.partial(layer_kernel, n_sp, n_local, small, large),
        out_shape=jax.ShapeDtypeStruct((rows, width), bf),
        in_specs=[vmem] * 7 + [anywhere] * 8,
        out_specs=vmem,
        scratch_shapes=scratch,
        compiler_params=pltpu.CompilerParams(
            collective_id=2, has_side_effects=True, vmem_limit_bytes=58 * 1024 * 1024
        ),
    )(resid, heads_in, v_large, turn_c, turn_s, gain, wts, wos, wol, wg, wu, wd, sg, su, sd)


def turn_table(positions, gain, width):
    channels = gain.shape[0]
    quarter, half = channels // 4, channels // 2
    inverse = 1.0 / rope_base ** (jnp.arange(quarter, dtype=jnp.float32) / quarter)
    by_row = (positions // GRID_W).astype(jnp.float32)[:, None] * inverse[None, :]
    by_column = (positions % GRID_W).astype(jnp.float32)[:, None] * inverse[None, :]
    angles = jnp.concatenate([by_row, by_row, by_column, by_column], axis=1)
    parted = gain.reshape(2, 2, quarter)
    facing = jnp.stack([-parted[:, 1], parted[:, 0]], axis=1).reshape(channels)
    copies = width // channels
    return (
        jnp.tile(jnp.cos(angles) * gain, (1, copies)),
        jnp.tile(jnp.sin(angles) * facing, (1, copies)),
    )


def dense_local(
    residual_in, q_small, k_small, v_small, q_large, k_large, v_large,
    gain_qs, gain_ks, gain_ql, gain_kl, w_out_small, w_out_large, g_ffn,
    routes, route_w, w_gate, w_up, w_down, ws_gate, ws_up, ws_down,
):
    local_rows = q_small.shape[0]
    positions = lax.axis_index("sp") * local_rows + jnp.arange(local_rows, dtype=jnp.int32)
    small, large = gain_qs.shape[0], gain_ql.shape[0]
    turns = [
        turn_table(positions, gain, width)
        for gain, width in (
            (gain_qs, q_small.shape[1]), (gain_ks, 128), (gain_ql, q_large.shape[1]), (gain_kl, large),
        )
    ]
    turn_c = jnp.concatenate([c for c, _ in turns], axis=1)
    turn_s = jnp.concatenate([v for _, v in turns], axis=1)
    heads_in = jnp.concatenate([q_small, k_small, v_small, q_large, k_large], axis=1)
    experts = w_gate.shape[0] * lax.axis_size("sp")
    named = routes[:, :, None] == jnp.arange(experts, dtype=jnp.int32)
    marks = jnp.sum(jnp.where(named, route_w[:, :, None], 0.0), axis=1)
    first = lax.reduce_precision(marks, 8, 7)
    second = lax.reduce_precision(marks - first, 8, 7)
    third = marks - first - second
    marks = jnp.concatenate([first, second, third], axis=1)
    marks = jnp.pad(marks, ((0, 0), (0, 128 - marks.shape[1]))).astype(jnp.bfloat16)
    return layer_call(
        small, large, residual_in, heads_in, v_large, turn_c, turn_s, g_ffn[None, :], marks, w_out_small, w_out_large,
        w_gate, w_up, w_down, ws_gate, ws_up, ws_down,
    )


def fits_dense(mesh, *arrays):
    routes, w_gate = arrays[14], arrays[16]
    tp = mesh.shape["tp"]
    if (arrays[7].shape[0], arrays[9].shape[0]) != (64, 128):
        return False
    if (arrays[2].shape[1], arrays[5].shape[1]) != (64 * tp, 128 * tp):
        return False
    ways = mesh.shape["sp"] * mesh.shape["tp"]
    rows_dev = routes.shape[0] // (ways * mesh.shape["grp"])
    experts = w_gate.shape[0]
    capacity = max(2, 2 * rows_dev * TOPK // experts)
    return mesh.shape["tp"] == 4 and capacity >= rows_dev and 3 * experts <= 128


def solution(mesh):
    placed = (
        P(("grp", "sp", "tp"), None),
        P(("grp", "sp"), "tp"),
        P(("grp", "sp"), "tp"),
        P(("grp", "sp"), "tp"),
        P(("grp", "sp"), "tp"),
        P(("grp", "sp"), "tp"),
        P(("grp", "sp"), "tp"),
        P(),
        P(),
        P(),
        P(),
        P("tp", None),
        P("tp", None),
        P(),
        P(("grp", "sp", "tp"), None),
        P(("grp", "sp", "tp"), None),
        P("sp", None, "tp"),
        P("sp", None, "tp"),
        P("sp", "tp", None),
        P(None, "tp"),
        P(None, "tp"),
        P("tp", None),
    )

    def whole(*arrays):
        body = dense_local if fits_dense(mesh, *arrays) else local
        return jax.shard_map(
            body, mesh=mesh, in_specs=placed, out_specs=P(("grp", "sp", "tp"), None), check_vma=False
        )(*arrays)

    return whole
```

```python
import functools
import math

import jax
import jax.numpy as jnp
from jax import lax
from jax.experimental import pallas as pl
from jax.experimental.pallas import tpu as pltpu
from jax.sharding import PartitionSpec as P

GRID_W = 64
TOPK = 4


norm_eps = 1e-06
rope_base = 10000.0
far_below = -1e30


def rotate_pairs(values, angles):
    front_half, back_half = jnp.split(values, 2, axis=-1)
    cosine_vals = jnp.cos(angles)[:, None, :]
    sine_vals = jnp.sin(angles)[:, None, :]
    return jnp.concatenate(
        [
            front_half * cosine_vals - back_half * sine_vals,
            front_half * sine_vals + back_half * cosine_vals,
        ],
        axis=-1,
    )


def norm_rotate(heads_in, gain, positions, grid_width):
    channels = gain.shape[0]
    values = heads_in.astype(jnp.float32).reshape(heads_in.shape[0], -1, channels)
    values = values * lax.rsqrt(jnp.mean(values * values, axis=-1, keepdims=True) + norm_eps) * gain
    quarter = channels // 4
    inverse = 1.0 / rope_base ** (jnp.arange(quarter, dtype=jnp.float32) / quarter)
    grid_rows = (positions // grid_width).astype(jnp.float32)
    grid_cols = (positions % grid_width).astype(jnp.float32)
    half_width = channels // 2
    turned = jnp.concatenate(
        [
            rotate_pairs(values[..., :half_width], grid_rows[:, None] * inverse[None, :]),
            rotate_pairs(values[..., half_width:], grid_cols[:, None] * inverse[None, :]),
        ],
        axis=-1,
    )
    return turned.astype(jnp.bfloat16)


def absorb(carried, segment, queries):
    peak_val, totals, mixture = carried
    kv_heads = queries.shape[1]
    channels = queries.shape[3]
    pairs = segment.reshape(segment.shape[0], 2, kv_heads, channels)
    scores = jnp.einsum(
        "qkgd,skd->kgqs", queries, pairs[:, 0], preferred_element_type=jnp.float32
    ) * channels ** (-0.5)
    new_peak = jnp.maximum(peak_val, jnp.max(scores, axis=-1))
    weights_raw = jnp.exp(scores - new_peak[..., None])
    shrink = jnp.exp(peak_val - new_peak)
    totals = totals * shrink + jnp.sum(weights_raw, axis=-1)
    update = jnp.einsum(
        "kgqs,skd->qkgd",
        weights_raw.astype(jnp.bfloat16),
        pairs[:, 1],
        preferred_element_type=jnp.float32,
    )
    mixture = mixture * jnp.transpose(shrink, (2, 0, 1))[..., None] + update
    return (new_peak, totals, mixture)


def absorb_blocks(carried, segment, queries):
    row_count = segment.shape[0]
    block_rows = math.gcd(row_count, 1024)
    stacked = segment.reshape(row_count // block_rows, block_rows, segment.shape[1])

    def fold_step(inner, key_block):
        return (absorb(inner, key_block, queries), None)

    carried, _ = lax.scan(fold_step, carried, stacked)
    return carried


def start_state(queries):
    local_rows, kv_heads, group, channels = queries.shape
    return (
        jnp.full((kv_heads, group, local_rows), far_below, jnp.float32),
        jnp.zeros((kv_heads, group, local_rows), jnp.float32),
        jnp.zeros(queries.shape, jnp.float32),
    )


def finish(carried):
    peak_val, totals, mixture = carried
    heads_out = mixture / jnp.transpose(totals, (2, 0, 1))[..., None]
    return heads_out.reshape(heads_out.shape[0], -1).astype(jnp.bfloat16)


def local(
    residual_in,
    q_small,
    k_small,
    v_small,
    q_large,
    k_large,
    v_large,
    gain_qs,
    gain_ks,
    gain_ql,
    gain_kl,
    w_out_small,
    w_out_large,
    g_ffn,
    routes,
    route_w,
    w_gate,
    w_up,
    w_down,
    ws_gate,
    ws_up,
    ws_down,
):
    local_rows = q_small.shape[0]
    positions = lax.axis_index("sp") * local_rows + jnp.arange(local_rows, dtype=jnp.int32)
    query_small = norm_rotate(q_small, gain_qs, positions, GRID_W)
    key_small = norm_rotate(k_small, gain_ks, positions, GRID_W)
    query_large = norm_rotate(q_large, gain_ql, positions, GRID_W)
    key_large = norm_rotate(k_large, gain_kl, positions, GRID_W)
    query_small = query_small.reshape(local_rows, key_small.shape[1], -1, gain_qs.shape[0])
    query_large = query_large.reshape(local_rows, key_large.shape[1], -1, gain_ql.shape[0])
    pack_small = jnp.concatenate([key_small.reshape(local_rows, -1), v_small], axis=1)
    pack_large = jnp.concatenate([key_large.reshape(local_rows, -1), v_large], axis=1)
    segment = (
        lax.all_gather(pack_small, "sp", axis=0, tiled=True),
        lax.all_gather(pack_large, "sp", axis=0, tiled=True),
    )
    heads_small = finish(absorb_blocks(start_state(query_small), segment[0], query_small))
    heads_large = finish(absorb_blocks(start_state(query_large), segment[1], query_large))
    tp_count = lax.axis_size("tp")
    sp_count = lax.axis_size("sp")
    rows_dev = local_rows // tp_count
    head_sum = lax.psum_scatter(
        (
            jnp.dot(heads_small, w_out_small, preferred_element_type=jnp.float32)
            + jnp.dot(heads_large, w_out_large, preferred_element_type=jnp.float32)
        ).astype(jnp.bfloat16),
        "tp",
        scatter_dimension=0,
        tiled=True,
    ).astype(jnp.float32)
    stream = (residual_in.astype(jnp.float32) + head_sum).astype(jnp.bfloat16)
    stream32 = lax.optimization_barrier(stream).astype(jnp.float32)
    normed = (
        stream32
        * lax.rsqrt(jnp.mean(stream32 * stream32, axis=-1, keepdims=True) + norm_eps)
        * g_ffn
    ).astype(jnp.bfloat16)
    channels = normed.shape[1]
    segment = lax.all_gather(normed, "tp", axis=0, tiled=True)
    gate_act = jnp.dot(segment, ws_gate, preferred_element_type=jnp.float32)
    up_act = jnp.dot(segment, ws_up, preferred_element_type=jnp.float32)
    hidden_shared = (jax.nn.silu(gate_act) * up_act).astype(jnp.bfloat16)
    shared = lax.psum_scatter(
        jnp.dot(hidden_shared, ws_down, preferred_element_type=jnp.float32).astype(jnp.bfloat16),
        "tp",
        scatter_dimension=0,
        tiled=True,
    ).astype(jnp.float32)
    local_experts = w_gate.shape[0]
    experts = local_experts * sp_count
    capacity = max(2, 2 * rows_dev * TOPK // experts)
    flat_ids = routes.reshape(-1)
    one_hot = (flat_ids[:, None] == jnp.arange(experts, dtype=jnp.int32)[None, :]).astype(jnp.int32)
    slot_ids = jnp.sum((jnp.cumsum(one_hot, axis=0) - 1) * one_hot, axis=1)
    targets = flat_ids * capacity + slot_ids
    owners = jnp.arange(rows_dev * TOPK, dtype=jnp.int32) // TOPK
    outbox = jnp.zeros((experts * capacity, channels), jnp.bfloat16).at[targets].set(normed[owners])
    arrived = lax.all_to_all(outbox, "sp", split_axis=0, concat_axis=0, tiled=True)
    arrived = lax.all_gather(
        arrived.reshape(sp_count, 1, local_experts, capacity, channels), "tp", axis=1, tiled=True
    )
    gate_act = jnp.einsum("abecd,edf->abecf", arrived, w_gate, preferred_element_type=jnp.float32)
    up_act = jnp.einsum("abecd,edf->abecf", arrived, w_up, preferred_element_type=jnp.float32)
    hidden = (jax.nn.silu(gate_act) * up_act).astype(jnp.bfloat16)
    partial_value = jnp.einsum(
        "abecf,efd->abecd", hidden, w_down, preferred_element_type=jnp.float32
    )
    summed = lax.psum_scatter(
        partial_value.astype(jnp.bfloat16), "tp", scatter_dimension=1, tiled=True
    )
    returned = lax.all_to_all(
        summed.reshape(sp_count * local_experts * capacity, channels),
        "sp",
        split_axis=0,
        concat_axis=0,
        tiled=True,
    )
    picked = returned[targets].reshape(rows_dev, TOPK, channels).astype(jnp.float32)
    routed = jnp.sum(picked * route_w[..., None], axis=1)
    return (stream32 + routed + shared).astype(jnp.bfloat16)


MESH = pl.DeviceIdType.MESH


def greet(peers):
    barrier = pltpu.get_barrier_semaphore()
    for peer in peers:
        pl.semaphore_signal(barrier, inc=1, device_id=peer, device_id_type=MESH)
    pl.semaphore_wait(barrier, len(peers))


def remote(src, dst, send, recv, peer):
    return pltpu.make_async_remote_copy(
        src_ref=src, dst_ref=dst, send_sem=send, recv_sem=recv, device_id=peer, device_id_type=MESH
    )


def f32dot(a, b):
    return jnp.dot(a, b, preferred_element_type=jnp.float32)


def rotated(tile, turn_c, turn_s, channels):
    lanes = tile.shape[1]
    row = lax.broadcasted_iota(jnp.int32, (lanes, lanes), 0)
    column = lax.broadcasted_iota(jnp.int32, (lanes, lanes), 1)
    swap = jnp.where((row ^ column) == channels // 4, 1.0, 0.0).astype(jnp.bfloat16)
    same = jnp.where((row ^ column) < channels, 1.0, 0.0).astype(jnp.bfloat16)
    wide = tile.astype(jnp.float32)
    square = wide * wide
    upper = square.astype(jnp.bfloat16)
    lower = (square - upper.astype(jnp.float32)).astype(jnp.bfloat16)
    mean = (f32dot(upper, same) + f32dot(lower, same)) * (1.0 / channels)
    return lax.rsqrt(mean + norm_eps) * (wide * turn_c + f32dot(tile, swap) * turn_s)


def attention(
    s, n_sp, small, large, heads_in, v_large, turn_c, turn_s,
    kv_own, kv, q_s, q_l, p_s, p_l, hs, hl, kvr, kup, kdown,
):
    rows = heads_in.shape[0]
    n_small, n_large = q_s.shape[0] // rows, q_l.shape[0] // rows

    def turned(start, channels):
        lanes = pl.ds(start, 128)
        return rotated(heads_in[:, lanes], turn_c[:, lanes], turn_s[:, lanes], channels)

    first = n_small * small
    mixed = turned(first, small)
    lane = lax.broadcasted_iota(jnp.int32, mixed.shape, 1)
    plain = heads_in[:, pl.ds(first, 128)].astype(jnp.float32)
    kv_own[:, 0:128] = jnp.where(lane < small, mixed, plain).astype(jnp.bfloat16)
    kv_own[:, 128:256] = turned(first + 128 + n_large * large, large).astype(jnp.bfloat16)
    kv_own[:, 256:384] = v_large[...]

    def send(source, row, sems, step, target):
        return pltpu.make_async_remote_copy(
            src_ref=source, dst_ref=kv.at[row], send_sem=sems.at[step], recv_sem=kvr.at[row],
            device_id={"sp": lax.rem(target + n_sp, n_sp)}, device_id_type=MESH,
        )

    @pl.when(s < n_sp - 1)
    def _():
        send(kv_own, s, kup, 0, s + 1).start()

    @pl.when(s > 0)
    def _():
        send(kv_own, s, kdown, 0, s - 1).start()

    kv[s] = kv_own[...]
    for tile in range(n_small * small // 128):
        both = turned(tile * 128, small).astype(jnp.bfloat16)
        for half in range(128 // small):
            q_s[pl.ds((tile * (128 // small) + half) * rows, rows), :] = both[:, half * small : (half + 1) * small]
    for tile in range(n_large):
        q_l[pl.ds(tile * rows, rows), :] = turned(first + 128 + tile * 128, large).astype(jnp.bfloat16)

    def score(row):
        span = pl.ds(pl.multiple_of(row * rows, rows), rows)
        keys = kv[row, :, 0:small]
        p_s[:, span] = lax.dot_general(
            q_s[...], keys, (((1,), (1,)), ((), ())), preferred_element_type=jnp.float32
        ) * small ** (-0.5)
        keys = kv[row, :, 128:256]
        p_l[:, span] = lax.dot_general(
            q_l[...], keys, (((1,), (1,)), ((), ())), preferred_element_type=jnp.float32
        ) * large ** (-0.5)

    score(s)

    @pl.loop(1, n_sp)
    def _(d):
        below, above = s - d, s + d

        @pl.when(below >= 0)
        def _():
            send(kv.at[below], below, kup, d, s + 1).wait_recv()

            @pl.when(s < n_sp - 1)
            def _():
                send(kv.at[below], below, kup, d, s + 1).start()

        @pl.when(above < n_sp)
        def _():
            send(kv.at[above], above, kdown, d, s - 1).wait_recv()

            @pl.when(s > 0)
            def _():
                send(kv.at[above], above, kdown, d, s - 1).start()

        @pl.when(below >= 0)
        def _():
            score(below)

        @pl.when(above < n_sp)
        def _():
            score(above)

    def head(index, scores, low, width, out):
        block = scores[pl.ds(index * rows, rows), :]
        raised = jnp.exp(block - jnp.max(block, axis=-1, keepdims=True))
        total = jnp.sum(raised, axis=-1, keepdims=True)
        weights = raised.astype(jnp.bfloat16)
        mixture = f32dot(weights[:, :rows], kv[0, :, low : low + width])
        for row in range(1, n_sp):
            mixture += f32dot(weights[:, row * rows : (row + 1) * rows], kv[row, :, low : low + width])
        out[:, index * width : (index + 1) * width] = (mixture / total).astype(jnp.bfloat16)

    for index in range(n_small):
        head(index, p_s, small, small, hs)
    for index in range(n_large):
        head(index, p_l, 256, large, hl)

    @pl.loop(0, n_sp)
    def _(d):
        @pl.when((s < n_sp - 1) & (s - d >= 0))
        def _():
            send(kv_own, s, kup, d, s + 1).wait_send()

        @pl.when((s > 0) & (s + d < n_sp))
        def _():
            send(kv_own, s, kdown, d, s - 1).wait_send()


def layer_kernel(
    n_sp, n_local, small, large, resid, heads_in, v_large, turn_c, turn_s, gain, wts, wos_h, wol_h, wg_h, wu_h, wd_h, sg_h, su_h, sd_h,
    out_ref,
    wos, wol, wg, wu, wd, sg, su, sd, kv_own, kv, q_s, q_l, p_s, p_l, hs, hl, part, pc, psx, px, blk, stream, gath, acc, ybuf, rc, sx, rx, sz, rz, own,
    wsem, kvr, kup, kdown, psend, precv, zsend, xsend, csend, grecv, ycs, ycr, yxs, yxr, yzs, yzr,
):
    s = lax.axis_index("sp")
    t = lax.axis_index("tp")
    rows, width = resid.shape
    xp = lax.rem(t + 2, 4)
    cp = t + 1 - 2 * lax.rem(t, 2)
    cxp = lax.rem(cp + 2, 4)
    peers = [{"sp": lax.rem(s + k, n_sp)} for k in range(1, n_sp)] + [{"tp": xp}, {"tp": cp}]
    loads = [
        pltpu.make_async_copy(src, dst, wsem.at[i])
        for i, (src, dst) in enumerate(
            ((wos_h, wos), (wol_h, wol), (sg_h, sg), (su_h, su), (sd_h, sd), (wg_h, wg), (wu_h, wu), (wd_h, wd))
        )
    ]
    greet(peers)
    for load in loads:
        load.start()

    def strip(index):
        return pl.ds(pl.multiple_of(index * rows, rows), rows)

    attention(
        s, n_sp, small, large, heads_in, v_large, turn_c, turn_s,
        kv_own, kv, q_s, q_l, p_s, p_l, hs, hl, kvr, kup, kdown,
    )
    loads[0].wait()
    loads[1].wait()
    part[...] = (f32dot(hs[...], wos[...]) + f32dot(hl[...], wol[...])).astype(jnp.bfloat16)
    to_x = remote(part.at[strip(cxp)], pc.at[1], psend.at[0], precv.at[0], {"tp": cp})
    to_own = remote(part.at[strip(cp)], pc.at[0], psend.at[1], precv.at[1], {"tp": cp})
    to_x.start()
    to_own.start()
    to_x.wait_recv()
    psx[...] = (part[strip(xp)].astype(jnp.float32) + pc[1].astype(jnp.float32)).astype(jnp.bfloat16)
    across = remote(psx, px, psend.at[2], precv.at[2], {"tp": xp})
    across.start()
    to_own.wait_recv()
    across.wait_recv()
    head_sum = part[strip(t)].astype(jnp.float32) + pc[0].astype(jnp.float32) + px[...].astype(jnp.float32)
    summed = (resid[...].astype(jnp.float32) + head_sum).astype(jnp.bfloat16)
    stream[...] = summed
    wide = summed.astype(jnp.float32)
    scale = lax.rsqrt(jnp.mean(wide * wide, axis=-1, keepdims=True) + norm_eps)
    blk[:, :width] = (wide * scale * gain[...]).astype(jnp.bfloat16)
    blk[:, width:] = wts[...]

    mine = gath.at[s, strip(t)]
    z_out = [
        remote(blk, mine, zsend.at[k], grecv.at[s, t], {"sp": lax.rem(s + k + 1, n_sp)})
        for k in range(n_sp - 1)
    ]
    x_own = remote(blk, mine, xsend.at[0], grecv.at[s, t], {"tp": xp})
    c_own = remote(blk, mine, csend.at[0, 0], grecv.at[s, t], {"tp": cp})
    x_own.start()
    for copy in z_out:
        copy.start()
    c_own.start()
    gath[s, strip(t)] = blk[...]
    for load in loads[2:]:
        load.wait()

    def block_of(k, column):
        row = lax.rem(s - k + n_sp, n_sp)
        return gath.at[row, strip(column)], grecv.at[row, column]

    def pass_on(k, column, send, peer):
        ref, sem = block_of(k, column)
        return remote(ref, ref, send, sem, peer)

    def core_part(k, slot):
        index = cp if slot == 0 else cxp
        return remote(ybuf.at[k, strip(index)], rc.at[k, slot], ycs.at[k, slot], ycr.at[k, slot], {"tp": cp})

    def x_part(k):
        return remote(sx.at[k], rx.at[k], yxs.at[k], yxr.at[k], {"tp": xp})

    def z_part(k):
        return remote(sz.at[k], rz.at[k], yzs.at[k], yzr.at[k], {"sp": lax.rem(s - k + n_sp, n_sp)})

    def spread(k):
        ahead = pass_on(k, t, xsend.at[k], {"tp": xp})
        ahead.wait_recv()
        ahead.start()
        pass_on(k, t, csend.at[k, 0], {"tp": cp}).start()

    if n_sp > 1:
        spread(1)

    @pl.loop(0, n_sp + 2)
    def _(step):
        @pl.when(step < n_sp - 2)
        def _():
            spread(step + 2)

        @pl.when(step < n_sp)
        def _():
            k = lax.rem(step + 1, n_sp)
            over = pass_on(k, xp, csend.at[k, 1], {"tp": cp})
            over.wait_recv()
            over.start()
            pass_on(k, cp, csend.at[k, 0], {"tp": cp}).wait_recv()
            pass_on(k, cxp, csend.at[k, 1], {"tp": cp}).wait_recv()
            row = lax.rem(s - k + n_sp, n_sp)
            tokens = gath[row, :, :width]
            marks = gath[row, :, width:].astype(jnp.float32)
            lane = lax.broadcasted_iota(jnp.int32, marks.shape, 1)

            @pl.when(k == 0)
            def _():
                gate = f32dot(tokens, sg[...])
                hidden = (gate / (1.0 + jnp.exp(-gate)) * f32dot(tokens, su[...])).astype(jnp.bfloat16)
                acc[...] = f32dot(hidden, sd[...])

            @pl.when(k > 0)
            def _():
                acc[...] = jnp.zeros_like(acc)

            experts = n_local * n_sp
            for e in range(n_local):
                number = s * n_local + e
                hit = (lane == number) | (lane == number + experts) | (lane == number + 2 * experts)
                weight = jnp.sum(jnp.where(hit, marks, 0.0), axis=1, keepdims=True)
                gate = f32dot(tokens, wg[e])
                hidden = (gate / (1.0 + jnp.exp(-gate)) * f32dot(tokens, wu[e])).astype(jnp.bfloat16)
                acc[...] += weight * f32dot(hidden, wd[e])
            ybuf[k] = acc[...].astype(jnp.bfloat16)
            core_part(k, 1).start()
            core_part(k, 0).start()

        @pl.when((step >= 1) & (step <= n_sp))
        def _():
            j = lax.rem(step, n_sp)
            core_part(j, 1).wait_recv()
            sx[j] = (ybuf[j, strip(xp)].astype(jnp.float32) + rc[j, 1].astype(jnp.float32)).astype(jnp.bfloat16)
            x_part(j).start()

        @pl.when(step >= 2)
        def _():
            j = lax.rem(step - 1, n_sp)
            core_part(j, 0).wait_recv()
            x_part(j).wait_recv()
            total = ybuf[j, strip(t)].astype(jnp.float32) + rc[j, 0].astype(jnp.float32) + rx[j].astype(jnp.float32)

            @pl.when(j > 0)
            def _():
                sz[j] = total.astype(jnp.bfloat16)
                z_part(j).start()

            @pl.when(j == 0)
            def _():
                own[...] = total

    result = stream[...].astype(jnp.float32) + own[...]
    for k in range(1, n_sp):
        z_part(k).wait_recv()
        result = result + rz[k].astype(jnp.float32)
    out_ref[...] = result.astype(jnp.bfloat16)

    to_x.wait_send()
    to_own.wait_send()
    across.wait_send()
    x_own.wait_send()
    c_own.wait_send()
    for copy in z_out:
        copy.wait_send()
    for k in range(n_sp):
        if k > 0:
            pass_on(k, t, xsend.at[k], {"tp": xp}).wait_send()
            pass_on(k, t, csend.at[k, 0], {"tp": cp}).wait_send()
            z_part(k).wait_send()
        pass_on(k, xp, csend.at[k, 1], {"tp": cp}).wait_send()
        core_part(k, 0).wait_send()
        core_part(k, 1).wait_send()
        x_part(k).wait_send()


def layer_call(small, large, resid, heads_in, v_large, turn_c, turn_s, gain, wts, wos, wol, wg, wu, wd, sg, su, sd):
    n_sp = lax.axis_size("sp")
    n_tp = lax.axis_size("tp")
    rows, width = resid.shape
    n_local = wg.shape[0]
    block = n_tp * rows
    padded = width + wts.shape[1]
    bf, f32 = jnp.bfloat16, jnp.float32
    dma = pltpu.SemaphoreType.DMA
    vmem = pl.BlockSpec(memory_space=pltpu.VMEM)
    anywhere = pl.BlockSpec(memory_space=pl.ANY)
    scratch = [pltpu.VMEM(w.shape, w.dtype) for w in (wos, wol, wg, wu, wd, sg, su, sd)] + [
        pltpu.VMEM((block, 384), bf),
        pltpu.VMEM((n_sp, block, 384), bf),
        pltpu.VMEM((wos.shape[0] // small * block, small), bf),
        pltpu.VMEM((wol.shape[0] // large * block, large), bf),
        pltpu.VMEM((wos.shape[0] // small * block, n_sp * block), f32),
        pltpu.VMEM((wol.shape[0] // large * block, n_sp * block), f32),
        pltpu.VMEM((block, wos.shape[0]), bf),
        pltpu.VMEM((block, wol.shape[0]), bf),
        pltpu.VMEM((n_tp * rows, width), bf),
        pltpu.VMEM((2, rows, width), bf),
        pltpu.VMEM((rows, width), bf),
        pltpu.VMEM((rows, width), bf),
        pltpu.VMEM((rows, padded), bf),
        pltpu.VMEM((rows, width), bf),
        pltpu.VMEM((n_sp, n_tp * rows, padded), bf),
        pltpu.VMEM((n_tp * rows, width), f32),
        pltpu.VMEM((n_sp, n_tp * rows, width), bf),
        pltpu.VMEM((n_sp, 2, rows, width), bf),
        pltpu.VMEM((n_sp, rows, width), bf),
        pltpu.VMEM((n_sp, rows, width), bf),
        pltpu.VMEM((n_sp, rows, width), bf),
        pltpu.VMEM((n_sp, rows, width), bf),
        pltpu.VMEM((rows, width), f32),
        dma((8,)), dma((n_sp,)), dma((n_sp,)), dma((n_sp,)), dma((3,)), dma((3,)),
        dma((n_sp - 1,)), dma((n_sp,)), dma((n_sp, 2)), dma((n_sp, n_tp)),
        dma((n_sp, 2)), dma((n_sp, 2)), dma((n_sp,)), dma((n_sp,)), dma((n_sp,)), dma((n_sp,)),
    ]
    return pl.pallas_call(
        functools.partial(layer_kernel, n_sp, n_local, small, large),
        out_shape=jax.ShapeDtypeStruct((rows, width), bf),
        in_specs=[vmem] * 7 + [anywhere] * 8,
        out_specs=vmem,
        scratch_shapes=scratch,
        compiler_params=pltpu.CompilerParams(
            collective_id=2, has_side_effects=True, vmem_limit_bytes=58 * 1024 * 1024
        ),
    )(resid, heads_in, v_large, turn_c, turn_s, gain, wts, wos, wol, wg, wu, wd, sg, su, sd)


def turn_table(positions, gain, width):
    channels = gain.shape[0]
    quarter, half = channels // 4, channels // 2
    inverse = 1.0 / rope_base ** (jnp.arange(quarter, dtype=jnp.float32) / quarter)
    by_row = (positions // GRID_W).astype(jnp.float32)[:, None] * inverse[None, :]
    by_column = (positions % GRID_W).astype(jnp.float32)[:, None] * inverse[None, :]
    angles = jnp.concatenate([by_row, by_row, by_column, by_column], axis=1)
    parted = gain.reshape(2, 2, quarter)
    facing = jnp.stack([-parted[:, 1], parted[:, 0]], axis=1).reshape(channels)
    copies = width // channels
    return (
        jnp.tile(jnp.cos(angles) * gain, (1, copies)),
        jnp.tile(jnp.sin(angles) * facing, (1, copies)),
    )


def dense_local(
    residual_in, q_small, k_small, v_small, q_large, k_large, v_large,
    gain_qs, gain_ks, gain_ql, gain_kl, w_out_small, w_out_large, g_ffn,
    routes, route_w, w_gate, w_up, w_down, ws_gate, ws_up, ws_down,
):
    local_rows = q_small.shape[0]
    positions = lax.axis_index("sp") * local_rows + jnp.arange(local_rows, dtype=jnp.int32)
    small, large = gain_qs.shape[0], gain_ql.shape[0]
    turns = [
        turn_table(positions, gain, width)
        for gain, width in (
            (gain_qs, q_small.shape[1]), (gain_ks, 128), (gain_ql, q_large.shape[1]), (gain_kl, large),
        )
    ]
    turn_c = jnp.concatenate([c for c, _ in turns], axis=1)
    turn_s = jnp.concatenate([v for _, v in turns], axis=1)
    heads_in = jnp.concatenate([q_small, k_small, v_small, q_large, k_large], axis=1)
    experts = w_gate.shape[0] * lax.axis_size("sp")
    named = routes[:, :, None] == jnp.arange(experts, dtype=jnp.int32)
    marks = jnp.sum(jnp.where(named, route_w[:, :, None], 0.0), axis=1)
    first = lax.reduce_precision(marks, 8, 7)
    second = lax.reduce_precision(marks - first, 8, 7)
    third = marks - first - second
    marks = jnp.concatenate([first, second, third], axis=1)
    marks = jnp.pad(marks, ((0, 0), (0, 128 - marks.shape[1]))).astype(jnp.bfloat16)
    return layer_call(
        small, large, residual_in, heads_in, v_large, turn_c, turn_s, g_ffn[None, :], marks, w_out_small, w_out_large,
        w_gate, w_up, w_down, ws_gate, ws_up, ws_down,
    )


def fits_dense(mesh, *arrays):
    routes, w_gate = arrays[14], arrays[16]
    tp = mesh.shape["tp"]
    if (arrays[7].shape[0], arrays[9].shape[0]) != (64, 128):
        return False
    if (arrays[2].shape[1], arrays[5].shape[1]) != (64 * tp, 128 * tp):
        return False
    ways = mesh.shape["sp"] * mesh.shape["tp"]
    rows_dev = routes.shape[0] // (ways * mesh.shape["grp"])
    experts = w_gate.shape[0]
    capacity = max(2, 2 * rows_dev * TOPK // experts)
    return mesh.shape["tp"] == 4 and capacity >= rows_dev and 3 * experts <= 128


def solution(mesh):
    placed = (
        P(("grp", "sp", "tp"), None),
        P(("grp", "sp"), "tp"),
        P(("grp", "sp"), "tp"),
        P(("grp", "sp"), "tp"),
        P(("grp", "sp"), "tp"),
        P(("grp", "sp"), "tp"),
        P(("grp", "sp"), "tp"),
        P(),
        P(),
        P(),
        P(),
        P("tp", None),
        P("tp", None),
        P(),
        P(("grp", "sp", "tp"), None),
        P(("grp", "sp", "tp"), None),
        P("sp", None, "tp"),
        P("sp", None, "tp"),
        P("sp", "tp", None),
        P(None, "tp"),
        P(None, "tp"),
        P("tp", None),
    )

    def whole(*arrays):
        body = dense_local if fits_dense(mesh, *arrays) else local
        return jax.shard_map(
            body, mesh=mesh, in_specs=placed, out_specs=P(("grp", "sp", "tp"), None), check_vma=False
        )(*arrays)

    return whole
```
